32 devices in a mesh: grp: 2 (over y), fs: 4 (over z), tp: 4 (over x, core).
Axes of the slice: x: 2, y: 2, z: 4, core: 2. Of those that a mesh axis runs over, the one named last changes fastest.
Arguments:
- tokens: bfloat16 [3072, 2048], P(('grp', 'fs'), 'tp'), parts along dimension 0, may hold values from -25 to 25
- gain_first: float32 [2048], replicated, may hold values from 0.1 to 1.9
- gate_first: bfloat16 [2048, 5120], P('fs', 'tp'), may hold values from -0.125 to 0.125
- up_first: bfloat16 [2048, 5120], P('fs', 'tp'), may hold values from -0.125 to 0.125
- down_first: bfloat16 [5120, 2048], P('tp', 'fs'), may hold values from -0.078125 to 0.078125
- gain_mixer: float32 [2048], replicated, may hold values from 0.1 to 1.9
- outer_gate: bfloat16 [2048, 1024], P('fs', 'tp'), may hold values from -0.125 to 0.125
- inner_gate: bfloat16 [2048, 1024], P('fs', 'tp'), may hold values from -0.125 to 0.125
- conv_input: bfloat16 [2048, 1024], P('fs', 'tp'), may hold values from -0.125 to 0.125
- conv_taps: float32 [3, 1024], P(None, 'tp'), may hold values from -3.5 to 3.5
- mixer_out: bfloat16 [1024, 2048], P('tp', 'fs'), may hold values from -0.1875 to 0.1875
- gain_last: float32 [2048], replicated, may hold values from 0.1 to 1.9
- gate_last: bfloat16 [2048, 5120], P('fs', 'tp'), may hold values from -0.125 to 0.125
- up_last: bfloat16 [2048, 5120], P('fs', 'tp'), may hold values from -0.125 to 0.125
- down_last: bfloat16 [5120, 2048], P('tp', 'fs'), may hold values from -0.078125 to 0.078125
Outputs:
- layer_out: bfloat16 [3072, 2048], P(('grp', 'fs'), 'tp'), parts along dimension 0
The draws below stay inside these ranges and needn't reach their ends.
There are 2 independent parts, one for each index of `grp`. The reference program is written for one: setup_inputs(seed, part) draws one part's arguments, and reference() takes and returns one part's arrays. A program takes and returns all parts, laid end to end along the dimension named above; an argument that names none is the same for every part. Nothing has to cross between parts.
All inputs are finite; a program needn't handle non-finite values.
Results may differ from the reference program's by a relative error of at most 0.015.
Values may be sent and summed in bfloat16 or wider, within the bound.
A program may use at most 64 MiB of HBM per device.

```python
import math
import jax
import jax.numpy as jnp
from jax import lax

D = 2048
FF = 5120
SC = 1024
KERNEL = 3
SEQ_LEN = 64
TOKENS = 1536
N_TP = 4


def draw_tokens(key, part):
    row_count = TOKENS
    col_count = D
    key_base, key_row, key_col = jax.random.split(jax.random.fold_in(key, 11), 3)
    values_raw = jnp.clip(jax.random.normal(key_base, (row_count, col_count), jnp.float32), -4.0, 4.0)
    row_scale = jnp.exp(jax.random.uniform(key_row, (row_count, 1), jnp.float32, math.log(0.5), math.log(2.0)))
    rising = 0.5 * jnp.power(4.0, jnp.arange(col_count, dtype=jnp.float32) / col_count)
    jitter = jnp.exp(jax.random.uniform(key_col, (col_count,), jnp.float32, -0.4, 0.4))
    return (values_raw * row_scale * (rising * jitter)[None, :]).astype(jnp.bfloat16)


def block_levels(key, shape, cuts, smallest, top_value):
    loudness = 1.0
    for position, shards_of in cuts:
        draws = jax.random.uniform(jax.random.fold_in(jax.random.fold_in(key, 6), position), (shards_of,), jnp.float32, smallest / len(cuts), top_value / len(cuts))
        loudness = loudness * jnp.repeat(jnp.exp(draws), shape[position] // shards_of).reshape((-1,) + (1,) * (len(shape) - 1 - position))
    return loudness


def scatter_about(key, shape, spread, limit, pieces=(), kind=jnp.bfloat16):
    drawn = spread * jax.random.normal(key, shape, jnp.float32)
    if pieces:
        drawn = drawn * block_levels(key, shape, pieces, -0.22, 0.18)
    return jnp.clip(drawn, -limit, limit).astype(kind)


def setup_inputs(seed: int = 0, part: int = 0) -> dict:
    key_of = jax.random.split(jax.random.key(seed), 16)
    part_keys = jax.random.split(jax.random.fold_in(key_of[15], part), 16)
    tokens = draw_tokens(jax.random.fold_in(jax.random.fold_in(key_of[15], part), 71), part)
    gain_first = jnp.clip(1.0 + 0.18 * jax.random.normal(key_of[1], (D,), jnp.float32), 0.1, 1.9)
    gate_first = scatter_about(key_of[2], (D, FF), D ** -0.5, 0.125, ((0, 4), (1, 4)))
    up_first = scatter_about(key_of[3], (D, FF), D ** -0.5, 0.125, ((0, 4), (1, 4)))
    down_first = scatter_about(key_of[4], (FF, D), FF ** -0.5, 0.078125, ((0, 4), (1, 4)))
    gain_mixer = jnp.clip(1.0 + 0.18 * jax.random.normal(key_of[5], (D,), jnp.float32), 0.1, 1.9)
    outer_gate = scatter_about(key_of[6], (D, SC), D ** -0.5, 0.125, ((0, 4), (1, 4)))
    inner_gate = scatter_about(key_of[7], (D, SC), D ** -0.5, 0.125, ((0, 4), (1, 4)))
    conv_input = scatter_about(key_of[8], (D, SC), D ** -0.5, 0.125, ((0, 4), (1, 4)))
    conv_taps = scatter_about(key_of[9], (KERNEL, SC), KERNEL ** -0.5, 3.5, ((1, 4),), jnp.float32)
    mixer_out = scatter_about(key_of[10], (SC, D), SC ** -0.5, 0.1875, ((0, 4), (1, 4)))
    gain_last = jnp.clip(1.0 + 0.18 * jax.random.normal(key_of[11], (D,), jnp.float32), 0.1, 1.9)
    gate_last = scatter_about(key_of[12], (D, FF), D ** -0.5, 0.125, ((0, 4), (1, 4)))
    up_last = scatter_about(key_of[13], (D, FF), D ** -0.5, 0.125, ((0, 4), (1, 4)))
    down_last = scatter_about(key_of[14], (FF, D), FF ** -0.5, 0.078125, ((0, 4), (1, 4)))
    return dict(tokens=tokens, gain_first=gain_first, gate_first=gate_first, up_first=up_first, down_first=down_first, gain_mixer=gain_mixer, outer_gate=outer_gate, inner_gate=inner_gate, conv_input=conv_input, conv_taps=conv_taps, mixer_out=mixer_out, gain_last=gain_last, gate_last=gate_last, up_last=up_last, down_last=down_last)


norm_eps = 1e-06

def rms_rows(residual, gain_vec):
    inverse = lax.rsqrt(lax.optimization_barrier(jnp.mean(residual * residual, axis=1, keepdims=True)) + norm_eps)
    return (residual * inverse * gain_vec).astype(jnp.bfloat16)

def blocked_sum(left_rows, right_rows):
    extent = left_rows.shape[1] // N_TP
    running = jnp.zeros((left_rows.shape[0], right_rows.shape[1]), jnp.float32)
    for block_id in range(N_TP):
        branch = jnp.dot(left_rows[:, block_id * extent:(block_id + 1) * extent], right_rows[block_id * extent:(block_id + 1) * extent], preferred_element_type=jnp.float32).astype(jnp.bfloat16)
        running = running + lax.optimization_barrier(branch).astype(jnp.float32)
    return running

def causal_mixing(gated, conv_taps):
    row_count, channels = gated.shape
    shaped = gated.reshape(row_count // SEQ_LEN, SEQ_LEN, channels)
    kernel = conv_taps.shape[0]
    padded = jnp.pad(shaped, ((0, 0), (kernel - 1, 0), (0, 0)))
    result = jnp.zeros_like(shaped)
    for offset in range(kernel):
        result = result + conv_taps[offset] * padded[:, offset:offset + SEQ_LEN]
    return result.reshape(row_count, channels)

def half_step(residual, gain_vec, gate_weight, up_weight, down_weight):
    normed = rms_rows(residual, gain_vec)
    gate_pre = jnp.dot(normed, gate_weight, preferred_element_type=jnp.float32)
    up_pre = jnp.dot(normed, up_weight, preferred_element_type=jnp.float32)
    hidden = (jax.nn.silu(gate_pre) * up_pre).astype(jnp.bfloat16)
    return residual + 0.5 * blocked_sum(hidden, down_weight)

def reference(tokens, gain_first, gate_first, up_first, down_first, gain_mixer, outer_gate, inner_gate, conv_input, conv_taps, mixer_out, gain_last, gate_last, up_last, down_last):
    residual = tokens.astype(jnp.float32)
    residual = half_step(residual, gain_first, gate_first, up_first, down_first)
    normed = rms_rows(residual, gain_mixer)
    outer_pre = jnp.dot(normed, outer_gate, preferred_element_type=jnp.float32)
    inner_pre = jnp.dot(normed, inner_gate, preferred_element_type=jnp.float32)
    value_pre = jnp.dot(normed, conv_input, preferred_element_type=jnp.float32)
    convolved = causal_mixing(inner_pre * value_pre, conv_taps)
    mixed_rows = (outer_pre * convolved).astype(jnp.bfloat16)
    residual = residual + blocked_sum(mixed_rows, mixer_out)
    residual = half_step(residual, gain_last, gate_last, up_last, down_last)
    return residual.astype(jnp.bfloat16)
```

```python
import functools

import jax
import jax.numpy as jnp
from jax import lax
from jax.experimental import pallas as pl
from jax.experimental.pallas import tpu as pltpu
from jax.sharding import PartitionSpec as P

SEQ_LEN = 64

VMEM_LIMIT = 63 * 2**20
LANES = 128
ROWS = 128
MESH = pl.DeviceIdType.MESH

norm_eps = 1e-06


def scaled_rows(residual, gain_vec, inverse):
    return (residual * inverse * gain_vec).astype(jnp.bfloat16)


def causal_mixing(gated, conv_taps):
    row_count, channels = gated.shape
    shaped = gated.reshape(row_count // SEQ_LEN, SEQ_LEN, channels)
    kernel = conv_taps.shape[0]
    padded = jnp.pad(shaped, ((0, 0), (kernel - 1, 0), (0, 0)))
    result = jnp.zeros_like(shaped)
    for offset in range(kernel):
        result = result + conv_taps[offset] * padded[:, offset : offset + SEQ_LEN]
    return result.reshape(row_count, channels)


def make_shards(groups, ring, parts):
    def shift(value, axis, size, by):
        return lax.ppermute(value, axis, [(i, (i + by) % size) for i in range(size)])

    def shards(
        tokens,
        gain_first,
        gate_first,
        up_first,
        down_first,
        gain_mixer,
        outer_gate,
        inner_gate,
        conv_input,
        conv_taps,
        mixer_out,
        gain_last,
        gate_last,
        up_last,
        down_last,
    ):
        column_count = tokens.shape[1]
        width = column_count * parts
        grain = width // (ring * groups)
        g = lax.axis_index("grp")
        z = lax.axis_index("fs")
        t = lax.axis_index("tp")

        def gather(batches, flights):
            pieces = {}
            landed = []
            for batch in batches:
                for name, (weight, axis) in batch.items():
                    pieces[name] = [weight]
                travelling = {
                    name: lax.dynamic_slice_in_dim(weight, g * grain, grain, axis)
                    for name, (weight, axis) in batch.items()
                }
                for _ in range(1, ring):
                    for name in batch:
                        block = travelling[name]
                        if len(landed) >= flights:
                            block, _ = lax.optimization_barrier((block, landed[-flights]))
                        block = shift(block, "fs", ring, 1)
                        landed.append(block)
                        travelling[name] = block
                        pieces[name].append(block)
                        for j in range(1, groups):
                            pieces[name].append(shift(block, "grp", groups, -j))
            return pieces

        def arrival_order(value):
            axis = value.ndim - 1
            blocks = [lax.dynamic_slice_in_dim(value, z * groups * grain, groups * grain, axis)]
            for r in range(1, ring):
                for j in range(groups):
                    start = ((z - r) % ring * groups + (g + j) % groups) * grain
                    blocks.append(lax.dynamic_slice_in_dim(value, start, grain, axis))
            return jnp.concatenate(blocks, axis)

        def own_columns(value, owner):
            blocks = []
            for k in range(column_count // grain):
                block = owner * (column_count // grain) + k
                shard, half = block // groups, block % groups
                turn = (z - shard) % ring
                place = turn * groups + jnp.where(turn == 0, half, (half - g) % groups)
                blocks.append(lax.dynamic_slice_in_dim(value, place * grain, grain, 1))
            return jnp.concatenate(blocks, 1)

        pieces = gather(
            (
                {"gate_first": (gate_first, 0), "up_first": (up_first, 0), "down_first": (down_first, 1)},
                {
                    "entries": (jnp.concatenate((outer_gate, inner_gate, conv_input), 1), 0),
                    "mixer_out": (mixer_out, 1),
                },
                {"gate_last": (gate_last, 0), "up_last": (up_last, 0), "down_last": (down_last, 1)},
            ),
            4,
        )

        def into(normed, pieces):
            total, start = 0.0, 0
            for piece in pieces:
                rows = normed[:, start : start + piece.shape[0]]
                total = total + jnp.dot(rows, piece, preferred_element_type=jnp.float32)
                start += piece.shape[0]
            return total

        def out_of(hidden, pieces):
            return jnp.concatenate(
                [
                    jnp.dot(hidden, piece, preferred_element_type=jnp.float32).astype(
                        jnp.bfloat16
                    )
                    for piece in pieces
                ],
                1,
            )

        def normalize(residual, gain_vec):
            inverse = lax.rsqrt(jnp.mean(residual * residual, axis=1, keepdims=True) + norm_eps)
            return scaled_rows(residual, gain_vec, inverse)

        def hidden_units(normed, gate_pieces, up_pieces):
            gate_pre, up_pre = into(normed, gate_pieces), into(normed, up_pieces)
            return (jax.nn.silu(gate_pre) * up_pre).astype(jnp.bfloat16)

        def add_branch(residual, branch, factor):
            return residual + factor * lax.psum(branch, "tp").astype(jnp.float32)

        residual = arrival_order(lax.all_gather(tokens, "tp", axis=1, tiled=True))
        residual = residual.astype(jnp.float32)

        normed = normalize(residual, arrival_order(gain_first))
        hidden = hidden_units(normed, pieces["gate_first"], pieces["up_first"])
        residual = add_branch(residual, out_of(hidden, pieces["down_first"]), 0.5)

        normed = normalize(residual, arrival_order(gain_mixer))
        channels = pieces["entries"][0].shape[1] // 3
        projected = into(normed, pieces["entries"])
        outer_pre, inner_pre, value_pre = (
            projected[:, i * channels : (i + 1) * channels] for i in range(3)
        )
        convolved = causal_mixing(inner_pre * value_pre, conv_taps)
        mixed_rows = (outer_pre * convolved).astype(jnp.bfloat16)
        residual = add_branch(residual, out_of(mixed_rows, pieces["mixer_out"]), 1.0)

        normed = normalize(residual, arrival_order(gain_last))
        hidden = hidden_units(normed, pieces["gate_last"], pieces["up_last"])
        branch = out_of(hidden, pieces["down_last"])
        total = own_columns(branch, t).astype(jnp.float32)
        for k in range(1, parts):
            theirs = own_columns(branch, (t + k) % parts)
            total = total + shift(theirs, "tp", parts, k).astype(jnp.float32)
        return (own_columns(residual, t) + 0.5 * total).astype(jnp.bfloat16)

    return shards


def layer_kernel(
    groups,
    ring,
    parts,
    tokens,
    gain_first,
    gain_mixer,
    gain_last,
    conv_taps,
    gate_first,
    up_first,
    down_first,
    outer_gate,
    inner_gate,
    conv_input,
    mixer_out,
    gate_last,
    up_last,
    down_last,
    out,
    in_first,
    out_first,
    in_mixer,
    out_mixer,
    in_last,
    out_last,
    spread,
    hidden,
    partial,
    core_got,
    side_sent,
    side_got,
    pair_sent,
    pair_got,
    kept,
    residual,
    weight_sent,
    weight_got,
    twin_sent,
    twin_got,
    own_got,
    token_sent,
    token_got,
    core_sems,
    side_sems,
    pair_sems,
):
    g, z, t = lax.axis_index("grp"), lax.axis_index("fs"), lax.axis_index("tp")
    half = lax.rem(z, 2)
    mate = z + 1 - 2 * half
    chip, core = lax.div(t, 2), lax.rem(t, 2)
    beside = (1 - chip) * 2 + core
    twin_core = chip * 2 + 1 - core
    rows, cols = tokens.shape
    chunks = rows // ROWS
    depth = gate_first.shape[0]
    side = depth // groups

    barrier = pltpu.get_barrier_semaphore()
    peers = [(g, lax.rem(z + d, ring), t) for d in range(1, ring)]
    peers += [(lax.rem(g + 1, groups), z, t), (g, z, beside), (g, z, twin_core)]
    for peer in peers:
        pl.semaphore_signal(barrier, inc=1, device_id=peer, device_id_type=MESH)
    pl.semaphore_wait(barrier, len(peers))

    def remote(src, dst, sent, got, peer):
        return pltpu.make_async_remote_copy(
            src_ref=src, dst_ref=dst, send_sem=sent, recv_sem=got, device_id=peer, device_id_type=MESH
        )

    stacks = (
        ((gate_first, in_first, 0), (up_first, in_first, 1), (down_first, out_first, None)),
        (
            (outer_gate, in_mixer, 0),
            (inner_gate, in_mixer, 1),
            (conv_input, in_mixer, 2),
            (mixer_out, out_mixer, None),
        ),
        ((gate_last, in_last, 0), (up_last, in_last, 1), (down_last, out_last, None)),
    )
    weights = [(b, entry) for b, stack in enumerate(stacks) for entry in stack]

    def source_view(entry, parity, begin, length):
        array, _, place = entry
        if place is None:
            extent = array.shape[0] // 2
            return array.at[pl.ds(parity * extent, extent), pl.ds(begin, length)]
        extent = array.shape[1] // 2
        return array.at[pl.ds(begin, length), pl.ds(parity * extent, extent)]

    def landing_view(entry, begin, length):
        array, landing, place = entry
        if place is None:
            return landing.at[:, pl.ds(begin, length)]
        extent = array.shape[1] // 2
        return landing.at[pl.ds(begin, length), pl.ds(place * extent, extent)]

    def aligned(value, unit):
        return pl.multiple_of(value, unit)

    def weight_copy(w, d):
        _, entry = weights[w]
        target = lax.rem(z + d, ring)
        return remote(
            source_view(entry, lax.rem(target, 2), aligned(g * side, side), side),
            landing_view(entry, aligned(z * depth + g * side, side), side),
            weight_sent.at[w, d - 1],
            weight_got.at[w, d - 1],
            (g, target, t),
        )

    def twin_copy(w, d):
        _, entry = weights[w]
        begin = aligned(lax.rem(z + ring - d, ring) * depth + g * side, side)
        view = landing_view(entry, begin, side)
        return remote(
            view, view, twin_sent.at[w, d - 1], twin_got.at[w, d - 1], (lax.rem(g + 1, groups), z, t)
        )

    def own_copy(w):
        _, entry = weights[w]
        return pltpu.make_async_copy(
            source_view(entry, half, 0, depth),
            landing_view(entry, aligned(z * depth, depth), depth),
            own_got.at[w],
        )

    hops = list(range(1, ring))

    def send_weights(names):
        for w in names:
            for d in hops:
                weight_copy(w, d).start()

    def pass_on(names):
        for w in names:
            for d in hops:
                weight_copy(w, d).wait_recv()
                twin_copy(w, d).start()

    def complete(names):
        for w in names:
            own_copy(w).wait()
            for d in hops:
                twin_copy(w, d).wait_recv()

    def token_copy(block, kind, k, column, whose, peer):
        view = spread.at[block, pl.ds(aligned(whose * rows + k * ROWS, ROWS), ROWS), pl.ds(aligned(column * cols, cols), cols)]
        return remote(view, view, token_sent.at[block, kind, k], token_got.at[block, kind, k], peer)

    to_mate, to_side, to_core = (g, mate, t), (g, z, beside), (g, z, twin_core)

    def token_out(block, kind, k):
        column, whose, peer = (
            (t, half, to_mate),
            (t, half, to_side),
            (t, 1 - half, to_side),
            (t, half, to_core),
            (t, 1 - half, to_core),
            (beside, half, to_core),
            (beside, 1 - half, to_core),
        )[kind]
        return token_copy(block, kind, k, column, whose, peer)

    def spread_out(block, gain):
        own_gain = gain[:, pl.ds(aligned(t * cols, cols), cols)]
        for k in range(chunks):
            piece = (residual[pl.ds(k * ROWS, ROWS), :] * own_gain).astype(jnp.bfloat16)
            spread[block, pl.ds(aligned(half * rows + k * ROWS, ROWS), ROWS), pl.ds(aligned(t * cols, cols), cols)] = piece
        for k in range(chunks):
            for kind in (0, 1, 3):
                token_out(block, kind, k).start()

    def spread_on(block):
        for k in range(chunks):
            token_out(block, 0, k).wait_recv()
            token_out(block, 2, k).start()
            token_out(block, 4, k).start()
        for first, second in ((1, 5), (2, 6)):
            for k in range(chunks):
                token_out(block, first, k).wait_recv()
                token_out(block, second, k).start()
        for kind in range(3, 7):
            for k in range(chunks):
                token_out(block, kind, k).wait_recv()
        for kind in range(7):
            for k in range(chunks):
                token_out(block, kind, k).wait_send()

    def row_start(i):
        whose = lax.rem(1 - half + lax.div(i, chunks), 2)
        return aligned(whose * rows + lax.rem(i, chunks) * ROWS, ROWS)

    def row_factor(lines, gain):
        plain = lines.astype(jnp.float32) * (1.0 / gain[...])
        return lax.rsqrt(jnp.mean(plain * plain, axis=1, keepdims=True) + norm_eps)

    def hidden_units(block, gain, landing):
        extent = landing.shape[1] // 2

        def step(i, carry):
            here = pl.ds(row_start(i), ROWS)
            lines = spread[block, here, :]
            both = jnp.dot(lines, landing[...], preferred_element_type=jnp.float32)
            both = both * row_factor(lines, gain)
            hidden[here, :] = (jax.nn.silu(both[:, :extent]) * both[:, extent:]).astype(jnp.bfloat16)
            return carry

        lax.fori_loop(0, 2 * chunks, step, 0)

    def mixed_rows(block, gain, landing, here):
        extent = landing.shape[1] // 3
        lines = spread[block, here, :]
        taps = conv_taps[:, pl.ds(aligned(half * extent, LANES), extent)]
        all_pre = jnp.dot(lines, landing[...], preferred_element_type=jnp.float32)
        all_pre = all_pre * row_factor(lines, gain)
        gated = all_pre[:, extent : 2 * extent] * all_pre[:, 2 * extent :]
        position = lax.rem(lax.broadcasted_iota(jnp.int32, gated.shape, 0), SEQ_LEN)
        count = taps.shape[0]
        convolved = taps[count - 1 : count, :] * gated
        for back in range(1, count):
            moved = jnp.where(position >= back, pltpu.roll(gated, back, 0), 0.0)
            convolved = convolved + taps[count - 1 - back : count - back, :] * moved
        return (all_pre[:, :extent] * convolved).astype(jnp.bfloat16)

    def branch(block, lines_of, landing, factor):
        def core_copy(i, c):
            here = pl.ds(row_start(i), ROWS)
            return remote(
                partial.at[here, pl.ds(aligned((2 * c + 1 - core) * cols, cols), cols)],
                core_got.at[block, here, pl.ds(c * cols, cols)],
                core_sems.at[block, 0, c, i],
                core_sems.at[block, 1, c, i],
                to_core,
            )

        def side_copy(i):
            here = pl.ds(row_start(i), ROWS)
            return remote(
                side_sent.at[here, :],
                side_got.at[block, here, :],
                side_sems.at[block, 0, i],
                side_sems.at[block, 1, i],
                to_side,
            )

        def pair_copy(k):
            here = pl.ds(aligned(k * ROWS, ROWS), ROWS)
            return remote(
                pair_sent.at[here, :],
                pair_got.at[block, here, :],
                pair_sems.at[block, 0, k],
                pair_sems.at[block, 1, k],
                to_mate,
            )

        def core_sum(i, which):
            here = pl.ds(row_start(i), ROWS)
            mine = partial[here, pl.ds(aligned((2 * which + core) * cols, cols), cols)]
            theirs = core_got[block, here, pl.ds(aligned(which * cols, cols), cols)]
            return mine.astype(jnp.float32) + theirs.astype(jnp.float32)

        def step(i, carry):
            @pl.when(i < 2 * chunks)
            def _():
                here = pl.ds(row_start(i), ROWS)
                partial[here, :] = jnp.dot(
                    lines_of(here), landing[...], preferred_element_type=jnp.float32
                ).astype(jnp.bfloat16)
                for c in range(2):
                    core_copy(i, c).start()

            @pl.when(jnp.logical_and(i >= 1, i < 2 * chunks + 1))
            def _():
                j = i - 1
                for c in range(2):
                    core_copy(j, c).wait_recv()
                side_sent[pl.ds(row_start(j), ROWS), :] = core_sum(j, 1 - chip).astype(jnp.bfloat16)
                side_copy(j).start()

            @pl.when(i >= 2)
            def _():
                j = i - 2
                side_copy(j).wait_recv()
                total = core_sum(j, chip) + side_got[block, pl.ds(row_start(j), ROWS), :].astype(jnp.float32)

                @pl.when(j < chunks)
                def _():
                    pair_sent[pl.ds(aligned(j * ROWS, ROWS), ROWS), :] = total.astype(jnp.bfloat16)
                    pair_copy(j).start()

                @pl.when(j >= chunks)
                def _():
                    kept[pl.ds(aligned((j - chunks) * ROWS, ROWS), ROWS), :] = total

            return carry

        lax.fori_loop(0, 2 * chunks + 2, step, 0)

        def last(k, carry):
            here = pl.ds(aligned(k * ROWS, ROWS), ROWS)
            pair_copy(k).wait_recv()
            total = kept[here, :] + pair_got[block, here, :].astype(jnp.float32)
            residual[here, :] = residual[here, :] + factor * total
            return carry

        lax.fori_loop(0, chunks, last, 0)

        def drain(i, carry):
            for c in range(2):
                core_copy(i, c).wait_send()
            side_copy(i).wait_send()

            @pl.when(i < chunks)
            def _():
                pair_copy(i).wait_send()

            return carry

        lax.fori_loop(0, 2 * chunks, drain, 0)

    entries = [[w for w, (b, e) in enumerate(weights) if b == block and e[2] is not None] for block in range(3)]
    exits = [[w for w, (b, e) in enumerate(weights) if b == block and e[2] is None] for block in range(3)]

    residual[...] = tokens[...].astype(jnp.float32)
    spread_out(0, gain_first)
    send_weights(entries[0] + exits[0] + entries[1] + exits[1] + entries[2][:1])
    for w in range(len(weights)):
        own_copy(w).start()
    spread_on(0)
    pass_on(entries[0])
    complete(entries[0])
    hidden_units(0, gain_first, in_first)
    pass_on(exits[0])
    complete(exits[0])
    branch(0, lambda here: hidden[here, :], out_first, 0.5)

    spread_out(1, gain_mixer)
    send_weights(entries[2][1:] + exits[2])
    pass_on(entries[1] + exits[1] + entries[2][:1])
    spread_on(1)
    complete(entries[1] + exits[1])
    pass_on(entries[2][1:])
    branch(1, functools.partial(mixed_rows, 1, gain_mixer, in_mixer), out_mixer, 1.0)

    spread_out(2, gain_last)
    pass_on(exits[2])
    spread_on(2)
    complete(entries[2])
    hidden_units(2, gain_last, in_last)
    complete(exits[2])
    branch(2, lambda here: hidden[here, :], out_last, 0.5)
    out[...] = residual[...].astype(out.dtype)

    for w in range(len(weights)):
        for d in hops:
            weight_copy(w, d).wait_send()
            twin_copy(w, d).wait_send()


def make_pair_shards(groups, ring, parts):
    def shards(
        tokens,
        gain_first,
        gate_first,
        up_first,
        down_first,
        gain_mixer,
        outer_gate,
        inner_gate,
        conv_input,
        conv_taps,
        mixer_out,
        gain_last,
        gate_last,
        up_last,
        down_last,
    ):
        rows, cols = tokens.shape
        width = cols * parts
        units, channels = gate_first.shape[1] // 2, outer_gate.shape[1] // 2
        count = 10
        chunks = rows // ROWS
        bf16, f32 = jnp.bfloat16, jnp.float32
        vmem = pl.BlockSpec(memory_space=pltpu.VMEM)
        hbm = pl.BlockSpec(memory_space=pl.ANY)
        dma = pltpu.SemaphoreType.DMA
        return pl.pallas_call(
            functools.partial(layer_kernel, groups, ring, parts),
            name="layer",
            out_shape=jax.ShapeDtypeStruct((rows, cols), bf16),
            in_specs=[vmem] * 5 + [hbm] * count,
            out_specs=vmem,
            scratch_shapes=[
                pltpu.VMEM((width, 2 * units), bf16),
                pltpu.VMEM((units, width), bf16),
                pltpu.VMEM((width, 3 * channels), bf16),
                pltpu.VMEM((channels, width), bf16),
                pltpu.VMEM((width, 2 * units), bf16),
                pltpu.VMEM((units, width), bf16),
                pltpu.VMEM((3, 2 * rows, width), bf16),
                pltpu.VMEM((2 * rows, units), bf16),
                pltpu.VMEM((2 * rows, width), bf16),
                pltpu.VMEM((3, 2 * rows, 2 * cols), bf16),
                pltpu.VMEM((2 * rows, cols), bf16),
                pltpu.VMEM((3, 2 * rows, cols), bf16),
                pltpu.VMEM((rows, cols), bf16),
                pltpu.VMEM((3, rows, cols), bf16),
                pltpu.VMEM((rows, cols), f32),
                pltpu.VMEM((rows, cols), f32),
                dma((count, ring - 1)),
                dma((count, ring - 1)),
                dma((count, ring - 1)),
                dma((count, ring - 1)),
                dma((count,)),
                dma((3, 7, chunks)),
                dma((3, 7, chunks)),
                dma((3, 2, 2, 2 * chunks)),
                dma((3, 2, 2 * chunks)),
                dma((3, 2, chunks)),
            ],
            compiler_params=pltpu.CompilerParams(
                collective_id=0, has_side_effects=True, vmem_limit_bytes=VMEM_LIMIT
            ),
        )(
            tokens,
            gain_first[None, :],
            gain_mixer[None, :],
            gain_last[None, :],
            conv_taps,
            gate_first,
            up_first,
            down_first,
            outer_gate,
            inner_gate,
            conv_input,
            mixer_out,
            gate_last,
            up_last,
            down_last,
        )

    return shards


def solution(mesh):
    in_specs = (
        P(("grp", "fs"), "tp"),
        P(),
        P("fs", "tp"),
        P("fs", "tp"),
        P("tp", "fs"),
        P(),
        P("fs", "tp"),
        P("fs", "tp"),
        P("fs", "tp"),
        P(None, "tp"),
        P("tp", "fs"),
        P(),
        P("fs", "tp"),
        P("fs", "tp"),
        P("tp", "fs"),
    )
    out_specs = P(("grp", "fs"), "tp")
    groups, ring, parts = mesh.shape["grp"], mesh.shape["fs"], mesh.shape["tp"]
    pair, general = make_pair_shards(groups, ring, parts), make_shards(groups, ring, parts)

    def shards(*args):
        rows, cols = args[0].shape
        depth, units = args[2].shape
        channels = args[6].shape[1]
        fits = (
            groups == 2
            and parts == 4
            and ring % 2 == 0
            and rows % ROWS == 0
            and ROWS % SEQ_LEN == 0
            and cols % LANES == 0
            and depth % (groups * LANES) == 0
            and units % (2 * LANES) == 0
            and channels % (2 * LANES) == 0
        )
        return (pair if fits else general)(*args)

    return jax.shard_map(shards, mesh=mesh, in_specs=in_specs, out_specs=out_specs, check_vma=False)
```

```python
import functools

import jax
import jax.numpy as jnp
from jax import lax
from jax.experimental import pallas as pl
from jax.experimental.pallas import tpu as pltpu
from jax.sharding import PartitionSpec as P

SEQ_LEN = 64

VMEM_LIMIT = 63 * 2**20
LANES = 128
MESH = pl.DeviceIdType.MESH

norm_eps = 1e-06


def scaled_rows(residual, gain_vec, inverse):
    return (residual * inverse * gain_vec).astype(jnp.bfloat16)


def causal_mixing(gated, conv_taps):
    row_count, channels = gated.shape
    shaped = gated.reshape(row_count // SEQ_LEN, SEQ_LEN, channels)
    kernel = conv_taps.shape[0]
    padded = jnp.pad(shaped, ((0, 0), (kernel - 1, 0), (0, 0)))
    result = jnp.zeros_like(shaped)
    for offset in range(kernel):
        result = result + conv_taps[offset] * padded[:, offset : offset + SEQ_LEN]
    return result.reshape(row_count, channels)


def make_shards(groups, ring, parts):
    def shift(value, axis, size, by):
        return lax.ppermute(value, axis, [(i, (i + by) % size) for i in range(size)])

    def shards(
        tokens,
        gain_first,
        gate_first,
        up_first,
        down_first,
        gain_mixer,
        outer_gate,
        inner_gate,
        conv_input,
        conv_taps,
        mixer_out,
        gain_last,
        gate_last,
        up_last,
        down_last,
    ):
        column_count = tokens.shape[1]
        width = column_count * parts
        grain = width // (ring * groups)
        g = lax.axis_index("grp")
        z = lax.axis_index("fs")
        t = lax.axis_index("tp")

        def gather(batches, flights):
            pieces = {}
            landed = []
            for batch in batches:
                for name, (weight, axis) in batch.items():
                    pieces[name] = [weight]
                travelling = {
                    name: lax.dynamic_slice_in_dim(weight, g * grain, grain, axis)
                    for name, (weight, axis) in batch.items()
                }
                for _ in range(1, ring):
                    for name in batch:
                        block = travelling[name]
                        if len(landed) >= flights:
                            block, _ = lax.optimization_barrier((block, landed[-flights]))
                        block = shift(block, "fs", ring, 1)
                        landed.append(block)
                        travelling[name] = block
                        pieces[name].append(block)
                        for j in range(1, groups):
                            pieces[name].append(shift(block, "grp", groups, -j))
            return pieces

        def arrival_order(value):
            axis = value.ndim - 1
            blocks = [lax.dynamic_slice_in_dim(value, z * groups * grain, groups * grain, axis)]
            for r in range(1, ring):
                for j in range(groups):
                    start = ((z - r) % ring * groups + (g + j) % groups) * grain
                    blocks.append(lax.dynamic_slice_in_dim(value, start, grain, axis))
            return jnp.concatenate(blocks, axis)

        def own_columns(value, owner):
            blocks = []
            for k in range(column_count // grain):
                block = owner * (column_count // grain) + k
                shard, half = block // groups, block % groups
                turn = (z - shard) % ring
                place = turn * groups + jnp.where(turn == 0, half, (half - g) % groups)
                blocks.append(lax.dynamic_slice_in_dim(value, place * grain, grain, 1))
            return jnp.concatenate(blocks, 1)

        pieces = gather(
            (
                {"gate_first": (gate_first, 0), "up_first": (up_first, 0), "down_first": (down_first, 1)},
                {
                    "entries": (jnp.concatenate((outer_gate, inner_gate, conv_input), 1), 0),
                    "mixer_out": (mixer_out, 1),
                },
                {"gate_last": (gate_last, 0), "up_last": (up_last, 0), "down_last": (down_last, 1)},
            ),
            4,
        )

        def into(normed, pieces):
            total, start = 0.0, 0
            for piece in pieces:
                rows = normed[:, start : start + piece.shape[0]]
                total = total + jnp.dot(rows, piece, preferred_element_type=jnp.float32)
                start += piece.shape[0]
            return total

        def out_of(hidden, pieces):
            return jnp.concatenate(
                [
                    jnp.dot(hidden, piece, preferred_element_type=jnp.float32).astype(
                        jnp.bfloat16
                    )
                    for piece in pieces
                ],
                1,
            )

        def normalize(residual, gain_vec):
            inverse = lax.rsqrt(jnp.mean(residual * residual, axis=1, keepdims=True) + norm_eps)
            return scaled_rows(residual, gain_vec, inverse)

        def hidden_units(normed, gate_pieces, up_pieces):
            gate_pre, up_pre = into(normed, gate_pieces), into(normed, up_pieces)
            return (jax.nn.silu(gate_pre) * up_pre).astype(jnp.bfloat16)

        def add_branch(residual, branch, factor):
            return residual + factor * lax.psum(branch, "tp").astype(jnp.float32)

        residual = arrival_order(lax.all_gather(tokens, "tp", axis=1, tiled=True))
        residual = residual.astype(jnp.float32)

        normed = normalize(residual, arrival_order(gain_first))
        hidden = hidden_units(normed, pieces["gate_first"], pieces["up_first"])
        residual = add_branch(residual, out_of(hidden, pieces["down_first"]), 0.5)

        normed = normalize(residual, arrival_order(gain_mixer))
        channels = pieces["entries"][0].shape[1] // 3
        projected = into(normed, pieces["entries"])
        outer_pre, inner_pre, value_pre = (
            projected[:, i * channels : (i + 1) * channels] for i in range(3)
        )
        convolved = causal_mixing(inner_pre * value_pre, conv_taps)
        mixed_rows = (outer_pre * convolved).astype(jnp.bfloat16)
        residual = add_branch(residual, out_of(mixed_rows, pieces["mixer_out"]), 1.0)

        normed = normalize(residual, arrival_order(gain_last))
        hidden = hidden_units(normed, pieces["gate_last"], pieces["up_last"])
        branch = out_of(hidden, pieces["down_last"])
        total = own_columns(branch, t).astype(jnp.float32)
        for k in range(1, parts):
            theirs = own_columns(branch, (t + k) % parts)
            total = total + shift(theirs, "tp", parts, k).astype(jnp.float32)
        return (own_columns(residual, t) + 0.5 * total).astype(jnp.bfloat16)

    return shards


def split_shard(extent):
    end = max(1, extent // LANES * 2 // 5) * LANES
    return extent - end, end


def layer_kernel(
    tokens,
    gain_first,
    gain_mixer,
    gain_last,
    conv_taps,
    gate_first,
    up_first,
    down_first,
    outer_gate,
    inner_gate,
    conv_input,
    mixer_out,
    gate_last,
    up_last,
    down_last,
    out,
    in_first,
    out_first,
    in_mixer,
    out_mixer,
    in_last,
    out_last,
    spread,
    hidden,
    mixed,
    partial,
    core_got,
    side_sent,
    side_got,
    pair_sent,
    pair_got,
    kept,
    residual,
    lift_in_first,
    lift_out_first,
    lift_in_mixer,
    lift_out_mixer,
    lift_in_last,
    lift_out_last,
    weight_sent,
    weight_got,
    twin_sent,
    twin_got,
    relay_sent,
    lift_got,
    own_got,
    token_sent,
    token_got,
    core_sems,
    side_sems,
    pair_sems,
):
    g, z, t = lax.axis_index("grp"), lax.axis_index("fs"), lax.axis_index("tp")
    half, pair = lax.rem(z, 2), lax.div(z, 2)
    mate = 2 * pair + 1 - half
    far_middle, far_end = 2 - pair, 3 * (1 - pair)
    middle = half != pair
    chip, core = lax.div(t, 2), lax.rem(t, 2)
    beside = (1 - chip) * 2 + core
    rows, cols = tokens.shape
    quarters = cols // LANES
    depth = gate_first.shape[0]
    to_mate, to_far_middle, to_far_end = (g, mate, t), (g, far_middle, t), (g, far_end, t)
    to_twin, to_side, to_core = (1 - g, z, t), (g, z, beside), (g, z, 2 * chip + 1 - core)

    barrier = pltpu.get_barrier_semaphore()
    peers = (to_mate, to_far_middle, to_far_end, to_twin, to_side, to_core)
    for peer in peers:
        pl.semaphore_signal(barrier, inc=1, device_id=peer, device_id_type=MESH)
    pl.semaphore_wait(barrier, len(peers))

    def remote(src, dst, sent, got, peer):
        return pltpu.make_async_remote_copy(
            src_ref=src, dst_ref=dst, send_sem=sent, recv_sem=got, device_id=peer, device_id_type=MESH
        )

    def aligned(value, unit):
        return pl.multiple_of(value, unit)

    entries = (
        ((gate_first, in_first, 0), (up_first, in_first, 1)),
        ((outer_gate, in_mixer, 0), (inner_gate, in_mixer, 1), (conv_input, in_mixer, 2)),
        ((gate_last, in_last, 0), (up_last, in_last, 1)),
    )
    exits = ((down_first, out_first), (mixer_out, out_mixer), (down_last, out_last))
    lifts = ((lift_in_first, lift_out_first), (lift_in_mixer, lift_out_mixer), (lift_in_last, lift_out_last))
    numbers, exit_base = [], []
    count = 0
    for entry in entries:
        numbers.append(list(range(count, count + len(entry))))
        exit_base.append(count + len(entry))
        count += len(entry) + quarters

    def entry_piece(block, n):
        array, landing, place = entries[block][n]
        split, side = split_shard(array.shape[1]), depth // 2

        def source(role, whole):
            lines = pl.ds(0, depth) if whole else pl.ds(aligned(g * side, side), side)
            return array.at[lines, pl.ds(role * split[0], split[role])]

        def target(role, origin, whole):
            begin = origin * depth if whole else origin * depth + g * side
            return landing.at[
                pl.ds(aligned(begin, side), depth if whole else side), pl.ds(place * split[role], split[role])
            ]

        return numbers[block][n], source, target, lifts[block][0].at[:, pl.ds(place * split[1], split[1])]

    def exit_piece(block, j):
        array, landing = exits[block]
        split = split_shard(array.shape[0])

        def source(role, whole):
            side = split[role] // 2
            begin = role * split[0] if whole else role * split[0] + g * side
            return array.at[
                pl.ds(begin if whole else aligned(begin, 8), split[role] if whole else side),
                pl.ds(aligned(j * LANES, LANES), LANES),
            ]

        def target(role, origin, whole):
            side = split[role] // 2
            place = lax.rem(origin, 2) * 2 + lax.div(origin, 2)
            lines = pl.ds(0, split[role]) if whole else pl.ds(aligned(g * side, side), side)
            return landing.at[j, lines, pl.ds(aligned(place * LANES, LANES), LANES)]

        return exit_base[block] + j, source, target, lifts[block][1].at[j]

    origins = (mate, far_middle, far_end)

    def on_each(*steps):
        for step in steps:
            step()

    def on_middle(*steps):
        pl.when(middle)(functools.partial(on_each, *steps))

    def on_end(*steps):
        pl.when(jnp.logical_not(middle))(functools.partial(on_each, *steps))

    def mate_middle(piece):
        w, source, target, _ = piece
        return remote(source(0, False), target(0, z, False), weight_sent.at[w, 0], weight_got.at[w, 0], to_mate)

    def lift_copy(piece):
        w, source, _, hold = piece
        return remote(source(1, False), hold, weight_sent.at[w, 1], lift_got.at[w], to_mate)

    def mate_end(piece):
        w, source, target, _ = piece
        return remote(source(1, False), target(1, z, False), weight_sent.at[w, 0], weight_got.at[w, 0], to_mate)

    def middle_copy(piece):
        w, source, target, _ = piece
        return remote(source(0, False), target(0, z, False), weight_sent.at[w, 1], weight_got.at[w, 1], to_far_middle)

    def end_copy(piece):
        w, source, target, _ = piece
        return remote(source(1, False), target(1, z, False), weight_sent.at[w, 2], weight_got.at[w, 1], to_far_end)

    def relay_middle(piece):
        w, _, target, _ = piece
        view = target(0, mate, False)
        return remote(view, view, relay_sent.at[w, 0], weight_got.at[w, 2], to_far_middle)

    def relay_end(piece):
        w, _, target, hold = piece
        return remote(hold, target(1, mate, False), relay_sent.at[w, 1], weight_got.at[w, 2], to_far_end)

    def twin_copy(piece, role, k):
        w, _, target, _ = piece
        view = target(role, origins[k], False)
        return remote(view, view, twin_sent.at[w, k], twin_got.at[w, k], to_twin)

    def own_copy(piece, role):
        w, source, target, _ = piece
        return pltpu.make_async_copy(source(role, True), target(role, z, True), own_got.at[w])

    def arrival(piece, role, k):
        w, _, target, _ = piece
        view = target(role, origins[k], False)
        return remote(view, view, weight_sent.at[w, 0], weight_got.at[w, k], to_mate)

    def send_near(pieces):
        for piece in pieces:
            on_middle(lambda: mate_end(piece).start())
            on_end(lambda: mate_middle(piece).start(), lambda: lift_copy(piece).start())

    def send_far(pieces):
        @pl.when(middle)
        def _():
            for piece in pieces:
                middle_copy(piece).start()
                end_copy(piece).start()

    def start_own(pieces):
        for piece in pieces:
            on_middle(lambda: own_copy(piece, 0).start())
            on_end(lambda: own_copy(piece, 1).start())

    def meet(pieces, k):
        @pl.when(middle)
        def _():
            for piece in pieces:
                arrival(piece, 0, k).wait_recv()
                if k == 0:
                    relay_middle(piece).start()
                    lift_copy(piece).wait_recv()
                    relay_end(piece).start()

        @pl.when(jnp.logical_not(middle))
        def _():
            for piece in pieces:
                arrival(piece, 1, k).wait_recv()

    def twin(pieces, k):
        for piece in pieces:
            on_middle(lambda: twin_copy(piece, 0, k).start())
            on_end(lambda: twin_copy(piece, 1, k).start())

    def pass_on(pieces, k):
        for piece in pieces:
            meet([piece], k)
            twin([piece], k)

    def complete(pieces):
        @pl.when(middle)
        def _():
            for piece in pieces:
                own_copy(piece, 0).wait()
                for k in (0, 1, 2):
                    twin_copy(piece, 0, k).wait_recv()

        @pl.when(jnp.logical_not(middle))
        def _():
            for piece in pieces:
                own_copy(piece, 1).wait()
                for k in (0, 1, 2):
                    twin_copy(piece, 1, k).wait_recv()

    def sent(pieces):
        @pl.when(middle)
        def _():
            for piece in pieces:
                for copy in (mate_end, middle_copy, end_copy, relay_middle, relay_end):
                    copy(piece).wait_send()
                for k in (0, 1, 2):
                    twin_copy(piece, 0, k).wait_send()

        @pl.when(jnp.logical_not(middle))
        def _():
            for piece in pieces:
                for copy in (mate_middle, lift_copy):
                    copy(piece).wait_send()
                for k in (0, 1, 2):
                    twin_copy(piece, 1, k).wait_send()

    into = [[entry_piece(b, n) for n in range(len(entries[b]))] for b in range(3)]
    outof = [[exit_piece(b, j) for j in range(quarters)] for b in range(3)]
    pieces = [into[b] + outof[b] for b in range(3)]

    def token_copy(block, kind, j):
        column, whose, peer = (
            (t, half, to_mate),
            (t, half, to_side),
            (t, 1 - half, to_side),
            (t, half, to_core),
            (t, 1 - half, to_core),
            (beside, half, to_core),
            (beside, 1 - half, to_core),
        )[kind]
        view = spread.at[
            block,
            pl.ds(aligned(whose * rows, rows), rows),
            pl.ds(aligned(column * cols + j * LANES, LANES), LANES),
        ]
        return remote(view, view, token_sent.at[block, kind, j], token_got.at[block, kind, j], peer)

    gains = (gain_first, gain_mixer, gain_last)

    def spread_out(block, j):
        place = pl.ds(aligned(t * cols + j * LANES, LANES), LANES)
        spread[block, pl.ds(aligned(half * rows, rows), rows), place] = (
            residual[j] * gains[block][:, place]
        ).astype(jnp.bfloat16)
        for kind in (0, 1, 3):
            token_copy(block, kind, j).start()

    def spread_mate(block):
        for j in range(quarters):
            token_copy(block, 0, j).wait_recv()
            token_copy(block, 2, j).start()
            token_copy(block, 4, j).start()

    def spread_side(block):
        for first, second in ((1, 5), (2, 6)):
            for j in range(quarters):
                token_copy(block, first, j).wait_recv()
                token_copy(block, second, j).start()
        for kind in range(3, 7):
            for j in range(quarters):
                token_copy(block, kind, j).wait_recv()

    def spread_sent(block):
        for kind in range(7):
            for j in range(quarters):
                token_copy(block, kind, j).wait_send()

    def row_factor(lines, gain):
        plain = lines.astype(jnp.float32) * (1.0 / gain[...])
        return lax.rsqrt(jnp.mean(plain * plain, axis=1, keepdims=True) + norm_eps)

    def hidden_units(block, landing, role):
        extent = split_shard(gate_first.shape[1])[role]

        def step(i, carry):
            here = pl.ds(aligned(i * rows, rows), rows)
            lines = spread[block, here, :]
            both = jnp.dot(lines, landing[:, : 2 * extent], preferred_element_type=jnp.float32)
            both = both * row_factor(lines, gains[block])
            hidden[here, :extent] = (jax.nn.silu(both[:, :extent]) * both[:, extent:]).astype(jnp.bfloat16)
            return carry

        lax.fori_loop(0, 2, step, 0)

    def mixed_rows(block, landing, role):
        split = split_shard(conv_taps.shape[1])
        extent = split[role]
        taps = conv_taps[:, role * split[0] : role * split[0] + extent]
        kernel = taps.shape[0]

        def step(i, carry):
            here = pl.ds(aligned(i * rows, rows), rows)
            lines = spread[block, here, :]
            all_pre = jnp.dot(lines, landing[:, : 3 * extent], preferred_element_type=jnp.float32)
            all_pre = all_pre * row_factor(lines, gains[block])
            gated = all_pre[:, extent : 2 * extent] * all_pre[:, 2 * extent : 3 * extent]
            position = lax.rem(lax.broadcasted_iota(jnp.int32, gated.shape, 0), SEQ_LEN)
            convolved = taps[kernel - 1 : kernel, :] * gated
            for back in range(1, kernel):
                moved = jnp.where(position >= back, pltpu.roll(gated, back, 0), 0.0)
                convolved = convolved + taps[kernel - 1 - back : kernel - back, :] * moved
            mixed[here, :extent] = (all_pre[:, :extent] * convolved).astype(jnp.bfloat16)
            return carry

        lax.fori_loop(0, 2, step, 0)

    def branch(block, lines, landing, factor, arriving, hooks):
        def core_copy(m):
            return remote(
                partial.at[m, :, pl.ds(aligned((1 - core) * 2 * LANES, LANES), 2 * LANES)],
                core_got.at[block, m],
                core_sems.at[block, 0, m],
                core_sems.at[block, 1, m],
                to_core,
            )

        def side_copy(m):
            return remote(
                side_sent.at[m],
                side_got.at[block, m],
                side_sems.at[block, 0, m],
                side_sems.at[block, 1, m],
                to_side,
            )

        def pair_copy(j):
            return remote(
                pair_sent.at[j],
                pair_got.at[block, j],
                pair_sems.at[block, 0, j],
                pair_sems.at[block, 1, j],
                to_mate,
            )

        def core_sum(m, which):
            mine = partial[m, :, pl.ds(aligned((core * 2 + which) * LANES, LANES), LANES)]
            theirs = core_got[block, m, :, pl.ds(aligned(which * LANES, LANES), LANES)]
            return mine.astype(jnp.float32) + theirs.astype(jnp.float32)

        total = 2 * quarters

        def step(i, carry):
            even = lax.rem(i, 2) == 0

            @pl.when(i < total)
            def _():
                j = lax.div(i, 2)
                if arriving:

                    @pl.when(jnp.logical_and(even, j < quarters - 1))
                    def _():
                        pass_on([exit_piece(block, j + 1)], 2)

                    @pl.when(even)
                    def _():
                        complete([exit_piece(block, j)])

                whose = lax.rem(lax.rem(i, 2) + 1 - half, 2)
                here = pl.ds(aligned(whose * rows, rows), rows)
                split = split_shard(exits[block][0].shape[0])

                def product(role):
                    extent = split[role]
                    partial[i] = jnp.dot(
                        lines[here, :extent], landing[j, :extent, :], preferred_element_type=jnp.float32
                    ).astype(jnp.bfloat16)

                on_middle(lambda: product(0))
                on_end(lambda: product(1))
                core_copy(i).start()

            @pl.when(jnp.logical_and(i >= 1, i < total + 1))
            def _():
                m = i - 1
                core_copy(m).wait_recv()
                side_sent[m] = core_sum(m, 1 - chip).astype(jnp.bfloat16)
                side_copy(m).start()

            @pl.when(jnp.logical_and(i >= 3, i < total + 3))
            def _():
                m = i - 3
                j = lax.div(m, 2)
                side_copy(m).wait_recv()
                summed = core_sum(m, chip) + side_got[block, m].astype(jnp.float32)

                @pl.when(lax.rem(m, 2) == 0)
                def _():
                    pair_sent[j] = summed.astype(jnp.bfloat16)
                    pair_copy(j).start()

                @pl.when(lax.rem(m, 2) == 1)
                def _():
                    kept[j] = summed

            @pl.when(jnp.logical_and(i >= 6, even))
            def _():
                j = lax.div(i - 6, 2)
                pair_copy(j).wait_recv()
                residual[j] = residual[j] + factor * (kept[j] + pair_got[block, j].astype(jnp.float32))
                if block < 2:
                    spread_out(block + 1, j)
                else:
                    out[:, pl.ds(aligned(j * LANES, LANES), LANES)] = residual[j].astype(out.dtype)

            for n, hook in hooks.items():
                pl.when(i == n)(hook)

            return carry

        if arriving:
            pass_on([exit_piece(block, 0)], 2)
        lax.fori_loop(0, total + 5, step, 0)

        def drain(m, carry):
            core_copy(m).wait_send()
            side_copy(m).wait_send()

            @pl.when(m < quarters)
            def _():
                pair_copy(m).wait_send()

            return carry

        lax.fori_loop(0, total, drain, 0)

    first, later = outof[0][: quarters // 2], outof[0][quarters // 2 :]
    send_near(first)
    send_far(first)
    send_near(into[0])
    send_far(into[0])
    for j in range(quarters):
        residual[j] = tokens[:, j * LANES : (j + 1) * LANES].astype(jnp.float32)
        spread_out(0, j)
    send_near(later)
    for b in range(3):
        start_own(pieces[b])
    send_near(pieces[1] + into[2][:1])
    on_end(lambda: send_near(into[2][1:]))

    for piece in first + into[0]:
        pass_on([piece], 0)
        pass_on([piece], 1)
    send_far(later)
    on_middle(lambda: spread_mate(0), lambda: pass_on(into[0], 2))
    on_end(lambda: pass_on(into[0], 2), lambda: spread_mate(0))
    spread_side(0)
    pass_on(later, 0)
    complete(into[0])
    send_far(pieces[1])
    on_middle(lambda: meet(pieces[1], 0))
    send_far(pieces[2])
    on_middle(lambda: hidden_units(0, in_first, 0))
    on_end(lambda: hidden_units(0, in_first, 1))
    pass_on(later, 1)
    hooks = {
        5: lambda: on_each(lambda: on_end(lambda: meet(pieces[1], 0)), lambda: twin(pieces[1], 0)),
        7: lambda: on_each(
            lambda: pass_on(pieces[1], 1),
            lambda: on_middle(lambda: pass_on(into[2], 0)),
            lambda: on_end(lambda: pass_on(into[2][:1], 0)),
        ),
    }
    branch(0, hidden, out_first, 0.5, True, hooks)

    on_end(lambda: send_near(outof[2]))
    on_middle(lambda: send_near(into[2][1:]))
    spread_mate(1)
    pass_on(pieces[1], 2)
    pass_on(into[2][:1], 1)
    spread_side(1)
    complete(pieces[1])
    on_middle(lambda: mixed_rows(1, in_mixer, 0))
    on_end(lambda: mixed_rows(1, in_mixer, 1))
    hooks = {
        2: lambda: pass_on(into[2][1:], 1),
        4: lambda: on_middle(lambda: send_near(outof[2][:1])),
        6: lambda: on_middle(lambda: send_near(outof[2][1:2])),
        7: lambda: on_each(
            lambda: on_middle(lambda: pass_on(outof[2], 0)), lambda: on_end(lambda: pass_on(into[2][1:], 0))
        ),
        8: lambda: on_middle(lambda: send_near(outof[2][2:3])),
        10: lambda: on_middle(lambda: send_near(outof[2][3:])),
        11: lambda: pass_on(outof[2], 1),
    }
    branch(1, mixed, out_mixer, 1.0, False, hooks)

    spread_mate(2)
    pass_on(into[2][:1], 2)
    spread_side(2)
    pass_on(into[2][1:], 2)
    on_end(lambda: pass_on(outof[2], 0))
    complete(into[2])
    on_middle(lambda: hidden_units(2, in_last, 0))
    on_end(lambda: hidden_units(2, in_last, 1))
    branch(2, hidden, out_last, 0.5, True, {})

    for block in range(3):
        spread_sent(block)
        sent(pieces[block])


def pair_shards(
    tokens,
    gain_first,
    gate_first,
    up_first,
    down_first,
    gain_mixer,
    outer_gate,
    inner_gate,
    conv_input,
    conv_taps,
    mixer_out,
    gain_last,
    gate_last,
    up_last,
    down_last,
):
    rows, cols = tokens.shape
    width = gain_first.shape[0]
    quarters, side = cols // LANES, gate_first.shape[0] // 2
    units, held_units = split_shard(gate_first.shape[1])
    channels, held_channels = split_shard(outer_gate.shape[1])
    bf16, f32 = jnp.bfloat16, jnp.float32
    vmem = pl.BlockSpec(memory_space=pltpu.VMEM)
    hbm = pl.BlockSpec(memory_space=pl.ANY)
    dma = pltpu.SemaphoreType.DMA
    count = 7 + 3 * quarters
    return pl.pallas_call(
        layer_kernel,
        name="layer",
        out_shape=jax.ShapeDtypeStruct((rows, cols), bf16),
        in_specs=[vmem] * 5 + [hbm] * 10,
        out_specs=vmem,
        scratch_shapes=[
            pltpu.VMEM((width, 2 * units), bf16),
            pltpu.VMEM((quarters, units, 4 * LANES), bf16),
            pltpu.VMEM((width, 3 * channels), bf16),
            pltpu.VMEM((quarters, channels, 4 * LANES), bf16),
            pltpu.VMEM((width, 2 * units), bf16),
            pltpu.VMEM((quarters, units, 4 * LANES), bf16),
            pltpu.VMEM((3, 2 * rows, width), bf16),
            pltpu.VMEM((2 * rows, units), bf16),
            pltpu.VMEM((2 * rows, channels), bf16),
            pltpu.VMEM((2 * quarters, rows, 4 * LANES), bf16),
            pltpu.VMEM((3, 2 * quarters, rows, 2 * LANES), bf16),
            pltpu.VMEM((2 * quarters, rows, LANES), bf16),
            pltpu.VMEM((3, 2 * quarters, rows, LANES), bf16),
            pltpu.VMEM((quarters, rows, LANES), bf16),
            pltpu.VMEM((3, quarters, rows, LANES), bf16),
            pltpu.VMEM((quarters, rows, LANES), f32),
            pltpu.VMEM((quarters, rows, LANES), f32),
            pltpu.VMEM((side, 2 * held_units), bf16),
            pltpu.VMEM((quarters, held_units // 2, LANES), bf16),
            pltpu.VMEM((side, 3 * held_channels), bf16),
            pltpu.VMEM((quarters, held_channels // 2, LANES), bf16),
            pltpu.VMEM((side, 2 * held_units), bf16),
            pltpu.VMEM((quarters, held_units // 2, LANES), bf16),
            dma((count, 3)),
            dma((count, 3)),
            dma((count, 3)),
            dma((count, 3)),
            dma((count, 2)),
            dma((count,)),
            dma((count,)),
            dma((3, 7, quarters)),
            dma((3, 7, quarters)),
            dma((3, 2, 2 * quarters)),
            dma((3, 2, 2 * quarters)),
            dma((3, 2, quarters)),
        ],
        compiler_params=pltpu.CompilerParams(
            collective_id=0, has_side_effects=True, vmem_limit_bytes=VMEM_LIMIT
        ),
    )(
        tokens,
        gain_first[None, :],
        gain_mixer[None, :],
        gain_last[None, :],
        conv_taps,
        gate_first,
        up_first,
        down_first,
        outer_gate,
        inner_gate,
        conv_input,
        mixer_out,
        gate_last,
        up_last,
        down_last,
    )


def solution(mesh):
    in_specs = (
        P(("grp", "fs"), "tp"),
        P(),
        P("fs", "tp"),
        P("fs", "tp"),
        P("tp", "fs"),
        P(),
        P("fs", "tp"),
        P("fs", "tp"),
        P("fs", "tp"),
        P(None, "tp"),
        P("tp", "fs"),
        P(),
        P("fs", "tp"),
        P("fs", "tp"),
        P("tp", "fs"),
    )
    out_specs = P(("grp", "fs"), "tp")
    groups, ring, parts = mesh.shape["grp"], mesh.shape["fs"], mesh.shape["tp"]
    general = make_shards(groups, ring, parts)

    def shards(*args):
        rows, cols = args[0].shape
        depth, units = args[2].shape
        channels = args[6].shape[1]
        fits = (
            groups == 2
            and parts == 4
            and ring == 4
            and rows % SEQ_LEN == 0
            and cols % LANES == 0
            and depth % (groups * LANES) == 0
            and units % (2 * LANES) == 0
            and channels % (2 * LANES) == 0
        )
        return (pair_shards if fits else general)(*args)

    return jax.shard_map(shards, mesh=mesh, in_specs=in_specs, out_specs=out_specs, check_vma=False)
```

```python
import functools

import jax
import jax.numpy as jnp
from jax import lax
from jax.experimental import pallas as pl
from jax.experimental.pallas import tpu as pltpu
from jax.sharding import PartitionSpec as P

SEQ_LEN = 64

VMEM_LIMIT = 63 * 2**20
LANES = 128
MESH = pl.DeviceIdType.MESH

norm_eps = 1e-06


def scaled_rows(residual, gain_vec, inverse):
    return (residual * inverse * gain_vec).astype(jnp.bfloat16)


def causal_mixing(gated, conv_taps):
    row_count, channels = gated.shape
    shaped = gated.reshape(row_count // SEQ_LEN, SEQ_LEN, channels)
    kernel = conv_taps.shape[0]
    padded = jnp.pad(shaped, ((0, 0), (kernel - 1, 0), (0, 0)))
    result = jnp.zeros_like(shaped)
    for offset in range(kernel):
        result = result + conv_taps[offset] * padded[:, offset : offset + SEQ_LEN]
    return result.reshape(row_count, channels)


def make_shards(groups, ring, parts):
    def shift(value, axis, size, by):
        return lax.ppermute(value, axis, [(i, (i + by) % size) for i in range(size)])

    def shards(
        tokens,
        gain_first,
        gate_first,
        up_first,
        down_first,
        gain_mixer,
        outer_gate,
        inner_gate,
        conv_input,
        conv_taps,
        mixer_out,
        gain_last,
        gate_last,
        up_last,
        down_last,
    ):
        column_count = tokens.shape[1]
        width = column_count * parts
        grain = width // (ring * groups)
        g = lax.axis_index("grp")
        z = lax.axis_index("fs")
        t = lax.axis_index("tp")

        def gather(batches, flights):
            pieces = {}
            landed = []
            for batch in batches:
                for name, (weight, axis) in batch.items():
                    pieces[name] = [weight]
                travelling = {
                    name: lax.dynamic_slice_in_dim(weight, g * grain, grain, axis)
                    for name, (weight, axis) in batch.items()
                }
                for _ in range(1, ring):
                    for name in batch:
                        block = travelling[name]
                        if len(landed) >= flights:
                            block, _ = lax.optimization_barrier((block, landed[-flights]))
                        block = shift(block, "fs", ring, 1)
                        landed.append(block)
                        travelling[name] = block
                        pieces[name].append(block)
                        for j in range(1, groups):
                            pieces[name].append(shift(block, "grp", groups, -j))
            return pieces

        def arrival_order(value):
            axis = value.ndim - 1
            blocks = [lax.dynamic_slice_in_dim(value, z * groups * grain, groups * grain, axis)]
            for r in range(1, ring):
                for j in range(groups):
                    start = ((z - r) % ring * groups + (g + j) % groups) * grain
                    blocks.append(lax.dynamic_slice_in_dim(value, start, grain, axis))
            return jnp.concatenate(blocks, axis)

        def own_columns(value, owner):
            blocks = []
            for k in range(column_count // grain):
                block = owner * (column_count // grain) + k
                shard, half = block // groups, block % groups
                turn = (z - shard) % ring
                place = turn * groups + jnp.where(turn == 0, half, (half - g) % groups)
                blocks.append(lax.dynamic_slice_in_dim(value, place * grain, grain, 1))
            return jnp.concatenate(blocks, 1)

        pieces = gather(
            (
                {"gate_first": (gate_first, 0), "up_first": (up_first, 0), "down_first": (down_first, 1)},
                {
                    "entries": (jnp.concatenate((outer_gate, inner_gate, conv_input), 1), 0),
                    "mixer_out": (mixer_out, 1),
                },
                {"gate_last": (gate_last, 0), "up_last": (up_last, 0), "down_last": (down_last, 1)},
            ),
            4,
        )

        def into(normed, pieces):
            total, start = 0.0, 0
            for piece in pieces:
                rows = normed[:, start : start + piece.shape[0]]
                total = total + jnp.dot(rows, piece, preferred_element_type=jnp.float32)
                start += piece.shape[0]
            return total

        def out_of(hidden, pieces):
            return jnp.concatenate(
                [
                    jnp.dot(hidden, piece, preferred_element_type=jnp.float32).astype(
                        jnp.bfloat16
                    )
                    for piece in pieces
                ],
                1,
            )

        def normalize(residual, gain_vec):
            inverse = lax.rsqrt(jnp.mean(residual * residual, axis=1, keepdims=True) + norm_eps)
            return scaled_rows(residual, gain_vec, inverse)

        def hidden_units(normed, gate_pieces, up_pieces):
            gate_pre, up_pre = into(normed, gate_pieces), into(normed, up_pieces)
            return (jax.nn.silu(gate_pre) * up_pre).astype(jnp.bfloat16)

        def add_branch(residual, branch, factor):
            return residual + factor * lax.psum(branch, "tp").astype(jnp.float32)

        residual = arrival_order(lax.all_gather(tokens, "tp", axis=1, tiled=True))
        residual = residual.astype(jnp.float32)

        normed = normalize(residual, arrival_order(gain_first))
        hidden = hidden_units(normed, pieces["gate_first"], pieces["up_first"])
        residual = add_branch(residual, out_of(hidden, pieces["down_first"]), 0.5)

        normed = normalize(residual, arrival_order(gain_mixer))
        channels = pieces["entries"][0].shape[1] // 3
        projected = into(normed, pieces["entries"])
        outer_pre, inner_pre, value_pre = (
            projected[:, i * channels : (i + 1) * channels] for i in range(3)
        )
        convolved = causal_mixing(inner_pre * value_pre, conv_taps)
        mixed_rows = (outer_pre * convolved).astype(jnp.bfloat16)
        residual = add_branch(residual, out_of(mixed_rows, pieces["mixer_out"]), 1.0)

        normed = normalize(residual, arrival_order(gain_last))
        hidden = hidden_units(normed, pieces["gate_last"], pieces["up_last"])
        branch = out_of(hidden, pieces["down_last"])
        total = own_columns(branch, t).astype(jnp.float32)
        for k in range(1, parts):
            theirs = own_columns(branch, (t + k) % parts)
            total = total + shift(theirs, "tp", parts, k).astype(jnp.float32)
        return (own_columns(residual, t) + 0.5 * total).astype(jnp.bfloat16)

    return shards


def split_shard(extent):
    end = max(1, extent // LANES * 2 // 5) * LANES
    return extent - end, end


def layer_kernel(
    tokens,
    gain_first,
    gain_mixer,
    gain_last,
    conv_taps,
    gate_first,
    up_first,
    down_first,
    outer_gate,
    inner_gate,
    conv_input,
    mixer_out,
    gate_last,
    up_last,
    down_last,
    out,
    in_first,
    out_first,
    in_mixer,
    out_mixer,
    in_last,
    out_last,
    spread,
    gated_pre,
    hidden,
    mixed,
    partial,
    core_got,
    side_sent,
    side_got,
    pair_sent,
    pair_got,
    kept,
    residual,
    lift_in_first,
    lift_out_first,
    lift_in_mixer,
    lift_out_mixer,
    lift_in_last,
    lift_out_last,
    weight_sent,
    weight_got,
    twin_sent,
    twin_got,
    relay_sent,
    lift_got,
    own_got,
    token_sent,
    token_got,
    core_sems,
    side_sems,
    pair_sems,
):
    g, z, t = lax.axis_index("grp"), lax.axis_index("fs"), lax.axis_index("tp")
    half, pair = lax.rem(z, 2), lax.div(z, 2)
    mate = 2 * pair + 1 - half
    far_middle, far_end = 2 - pair, 3 * (1 - pair)
    middle = half != pair
    chip, core = lax.div(t, 2), lax.rem(t, 2)
    beside = (1 - chip) * 2 + core
    rows, cols = tokens.shape
    quarters = cols // LANES
    depth = gate_first.shape[0]
    to_mate, to_far_middle, to_far_end = (g, mate, t), (g, far_middle, t), (g, far_end, t)
    to_twin, to_side, to_core = (1 - g, z, t), (g, z, beside), (g, z, 2 * chip + 1 - core)

    barrier = pltpu.get_barrier_semaphore()
    peers = (to_mate, to_far_middle, to_far_end, to_twin, to_side, to_core)
    for peer in peers:
        pl.semaphore_signal(barrier, inc=1, device_id=peer, device_id_type=MESH)
    pl.semaphore_wait(barrier, len(peers))

    def remote(src, dst, sent, got, peer):
        return pltpu.make_async_remote_copy(
            src_ref=src, dst_ref=dst, send_sem=sent, recv_sem=got, device_id=peer, device_id_type=MESH
        )

    def aligned(value, unit):
        return pl.multiple_of(value, unit)

    entries = (
        ((gate_first, in_first, 0), (up_first, in_first, 1)),
        ((outer_gate, in_mixer, 0), (inner_gate, in_mixer, 1), (conv_input, in_mixer, 2)),
        ((gate_last, in_last, 0), (up_last, in_last, 1)),
    )
    exits = ((down_first, out_first), (mixer_out, out_mixer), (down_last, out_last))
    lifts = ((lift_in_first, lift_out_first), (lift_in_mixer, lift_out_mixer), (lift_in_last, lift_out_last))
    numbers, exit_base = [], []
    count = 0
    for entry in entries:
        numbers.append(list(range(count, count + len(entry))))
        exit_base.append(count + len(entry))
        count += len(entry) + quarters

    def entry_piece(block, n):
        array, landing, place = entries[block][n]
        split, side = split_shard(array.shape[1]), depth // 2

        def source(role, whole):
            lines = pl.ds(0, depth) if whole else pl.ds(aligned(g * side, side), side)
            return array.at[lines, pl.ds(role * split[0], split[role])]

        def target(role, origin, whole):
            begin = origin * depth if whole else origin * depth + g * side
            return landing.at[
                pl.ds(aligned(begin, side), depth if whole else side), pl.ds(place * split[role], split[role])
            ]

        return numbers[block][n], source, target, lifts[block][0].at[:, pl.ds(place * split[1], split[1])]

    def exit_piece(block, j):
        array, landing = exits[block]
        split = split_shard(array.shape[0])

        def source(role, whole):
            side = split[role] // 2
            begin = role * split[0] if whole else role * split[0] + g * side
            return array.at[
                pl.ds(begin if whole else aligned(begin, 8), split[role] if whole else side),
                pl.ds(aligned(j * LANES, LANES), LANES),
            ]

        def target(role, origin, whole):
            side = split[role] // 2
            place = lax.rem(origin, 2) * 2 + lax.div(origin, 2)
            lines = pl.ds(0, split[role]) if whole else pl.ds(aligned(g * side, side), side)
            return landing.at[j, lines, pl.ds(aligned(place * LANES, LANES), LANES)]

        return exit_base[block] + j, source, target, lifts[block][1].at[j]

    origins = (mate, far_middle, far_end)

    def on_each(*steps):
        for step in steps:
            step()

    def on_middle(*steps):
        pl.when(middle)(functools.partial(on_each, *steps))

    def on_end(*steps):
        pl.when(jnp.logical_not(middle))(functools.partial(on_each, *steps))

    def mate_middle(piece):
        w, source, target, _ = piece
        return remote(source(0, False), target(0, z, False), weight_sent.at[w, 0], weight_got.at[w, 0], to_mate)

    def lift_copy(piece):
        w, source, _, hold = piece
        return remote(source(1, False), hold, weight_sent.at[w, 1], lift_got.at[w], to_mate)

    def mate_end(piece):
        w, source, target, _ = piece
        return remote(source(1, False), target(1, z, False), weight_sent.at[w, 0], weight_got.at[w, 0], to_mate)

    def middle_copy(piece):
        w, source, target, _ = piece
        return remote(source(0, False), target(0, z, False), weight_sent.at[w, 1], weight_got.at[w, 1], to_far_middle)

    def end_copy(piece):
        w, source, target, _ = piece
        return remote(source(1, False), target(1, z, False), weight_sent.at[w, 2], weight_got.at[w, 1], to_far_end)

    def relay_middle(piece):
        w, _, target, _ = piece
        view = target(0, mate, False)
        return remote(view, view, relay_sent.at[w, 0], weight_got.at[w, 2], to_far_middle)

    def relay_end(piece):
        w, _, target, hold = piece
        return remote(hold, target(1, mate, False), relay_sent.at[w, 1], weight_got.at[w, 2], to_far_end)

    def twin_copy(piece, role, k):
        w, _, target, _ = piece
        view = target(role, origins[k], False)
        return remote(view, view, twin_sent.at[w, k], twin_got.at[w, k], to_twin)

    def own_copy(piece, role):
        w, source, target, _ = piece
        return pltpu.make_async_copy(source(role, True), target(role, z, True), own_got.at[w])

    def arrival(piece, role, k):
        w, _, target, _ = piece
        view = target(role, origins[k], False)
        return remote(view, view, weight_sent.at[w, 0], weight_got.at[w, k], to_mate)

    def send_near(pieces):
        for piece in pieces:
            on_middle(lambda: mate_end(piece).start())
            on_end(lambda: mate_middle(piece).start(), lambda: lift_copy(piece).start())

    def send_far(pieces):
        @pl.when(middle)
        def _():
            for piece in pieces:
                middle_copy(piece).start()
                end_copy(piece).start()

    def start_own(pieces):
        for piece in pieces:
            on_middle(lambda: own_copy(piece, 0).start())
            on_end(lambda: own_copy(piece, 1).start())

    def meet(pieces, k):
        @pl.when(middle)
        def _():
            for piece in pieces:
                arrival(piece, 0, k).wait_recv()
                if k == 0:
                    relay_middle(piece).start()
                    lift_copy(piece).wait_recv()
                    relay_end(piece).start()

        @pl.when(jnp.logical_not(middle))
        def _():
            for piece in pieces:
                arrival(piece, 1, k).wait_recv()

    def twin(pieces, k):
        for piece in pieces:
            on_middle(lambda: twin_copy(piece, 0, k).start())
            on_end(lambda: twin_copy(piece, 1, k).start())

    def pass_on(pieces, k):
        for piece in pieces:
            meet([piece], k)
            twin([piece], k)

    def complete(pieces):
        @pl.when(middle)
        def _():
            for piece in pieces:
                own_copy(piece, 0).wait()
                for k in (0, 1, 2):
                    twin_copy(piece, 0, k).wait_recv()

        @pl.when(jnp.logical_not(middle))
        def _():
            for piece in pieces:
                own_copy(piece, 1).wait()
                for k in (0, 1, 2):
                    twin_copy(piece, 1, k).wait_recv()

    def sent(pieces):
        @pl.when(middle)
        def _():
            for piece in pieces:
                for copy in (mate_end, middle_copy, end_copy, relay_middle, relay_end):
                    copy(piece).wait_send()
                for k in (0, 1, 2):
                    twin_copy(piece, 0, k).wait_send()

        @pl.when(jnp.logical_not(middle))
        def _():
            for piece in pieces:
                for copy in (mate_middle, lift_copy):
                    copy(piece).wait_send()
                for k in (0, 1, 2):
                    twin_copy(piece, 1, k).wait_send()

    into = [[entry_piece(b, n) for n in range(len(entries[b]))] for b in range(3)]
    outof = [[exit_piece(b, j) for j in range(quarters)] for b in range(3)]
    pieces = [into[b] + outof[b] for b in range(3)]

    def token_copy(block, kind, j):
        column, whose, peer = (
            (t, half, to_mate),
            (t, half, to_side),
            (t, 1 - half, to_side),
            (t, half, to_core),
            (t, 1 - half, to_core),
            (beside, half, to_core),
            (beside, 1 - half, to_core),
        )[kind]
        view = spread.at[
            block,
            pl.ds(aligned(whose * rows, rows), rows),
            pl.ds(aligned(column * cols + j * LANES, LANES), LANES),
        ]
        return remote(view, view, token_sent.at[block, kind, j], token_got.at[block, kind, j], peer)

    gains = (gain_first, gain_mixer, gain_last)

    def spread_out(block, j):
        place = pl.ds(aligned(t * cols + j * LANES, LANES), LANES)
        spread[block, pl.ds(aligned(half * rows, rows), rows), place] = (
            residual[j] * gains[block][:, place]
        ).astype(jnp.bfloat16)
        for kind in (0, 1, 3):
            token_copy(block, kind, j).start()

    def spread_mate(block):
        for j in range(quarters):
            token_copy(block, 0, j).wait_recv()
            token_copy(block, 2, j).start()
            token_copy(block, 4, j).start()

    def spread_side(block):
        for first, second in ((1, 5), (2, 6)):
            for j in range(quarters):
                token_copy(block, first, j).wait_recv()
                token_copy(block, second, j).start()
        for kind in range(3, 7):
            for j in range(quarters):
                token_copy(block, kind, j).wait_recv()

    def spread_sent(block):
        for kind in range(7):
            for j in range(quarters):
                token_copy(block, kind, j).wait_send()

    def row_factor(lines, gain):
        plain = lines.astype(jnp.float32) * (1.0 / gain[...])
        return lax.rsqrt(jnp.mean(plain * plain, axis=1, keepdims=True) + norm_eps)

    def gate_units(block, landing, role):
        extent = split_shard(gate_first.shape[1])[role]

        def step(i, carry):
            here = pl.ds(aligned(i * rows, rows), rows)
            lines = spread[block, here, :]
            pre = jnp.dot(lines, landing[:, :extent], preferred_element_type=jnp.float32)
            gated_pre[here, :extent] = pre * row_factor(lines, gains[block])
            return carry

        lax.fori_loop(0, 2, step, 0)

    def hidden_units(block, landing, role):
        extent = split_shard(gate_first.shape[1])[role]

        def step(i, carry):
            here = pl.ds(aligned(i * rows, rows), rows)
            lines = spread[block, here, :]
            pre = jnp.dot(lines, landing[:, extent : 2 * extent], preferred_element_type=jnp.float32)
            pre = pre * row_factor(lines, gains[block])
            hidden[here, :extent] = (jax.nn.silu(gated_pre[here, :extent]) * pre).astype(jnp.bfloat16)
            return carry

        lax.fori_loop(0, 2, step, 0)

    def mixed_rows(block, landing, role):
        split = split_shard(conv_taps.shape[1])
        extent = split[role]
        taps = conv_taps[:, role * split[0] : role * split[0] + extent]
        kernel = taps.shape[0]

        def step(i, carry):
            here = pl.ds(aligned(i * rows, rows), rows)
            lines = spread[block, here, :]
            all_pre = jnp.dot(lines, landing[:, : 3 * extent], preferred_element_type=jnp.float32)
            all_pre = all_pre * row_factor(lines, gains[block])
            gated = all_pre[:, extent : 2 * extent] * all_pre[:, 2 * extent : 3 * extent]
            position = lax.rem(lax.broadcasted_iota(jnp.int32, gated.shape, 0), SEQ_LEN)
            convolved = taps[kernel - 1 : kernel, :] * gated
            for back in range(1, kernel):
                moved = jnp.where(position >= back, pltpu.roll(gated, back, 0), 0.0)
                convolved = convolved + taps[kernel - 1 - back : kernel - back, :] * moved
            mixed[here, :extent] = (all_pre[:, :extent] * convolved).astype(jnp.bfloat16)
            return carry

        lax.fori_loop(0, 2, step, 0)

    def branch(block, lines, landing, factor, arriving, hooks):
        def core_copy(m):
            return remote(
                partial.at[m, :, pl.ds(aligned((1 - core) * 2 * LANES, LANES), 2 * LANES)],
                core_got.at[block, m],
                core_sems.at[block, 0, m],
                core_sems.at[block, 1, m],
                to_core,
            )

        def side_copy(m):
            return remote(
                side_sent.at[m],
                side_got.at[block, m],
                side_sems.at[block, 0, m],
                side_sems.at[block, 1, m],
                to_side,
            )

        def pair_copy(j):
            return remote(
                pair_sent.at[j],
                pair_got.at[block, j],
                pair_sems.at[block, 0, j],
                pair_sems.at[block, 1, j],
                to_mate,
            )

        def core_sum(m, which):
            mine = partial[m, :, pl.ds(aligned((core * 2 + which) * LANES, LANES), LANES)]
            theirs = core_got[block, m, :, pl.ds(aligned(which * LANES, LANES), LANES)]
            return mine.astype(jnp.float32) + theirs.astype(jnp.float32)

        total = 2 * quarters

        def step(i, carry):
            even = lax.rem(i, 2) == 0

            @pl.when(i < total)
            def _():
                j = lax.div(i, 2)
                if arriving == "late":

                    @pl.when(jnp.logical_and(even, jnp.logical_and(j >= quarters // 2 - 1, j < quarters - 1)))
                    def _():
                        pass_on([exit_piece(block, j + 1)], 2)

                if arriving:

                    @pl.when(even)
                    def _():
                        complete([exit_piece(block, j)])

                whose = lax.rem(lax.rem(i, 2) + 1 - half, 2)
                here = pl.ds(aligned(whose * rows, rows), rows)
                split = split_shard(exits[block][0].shape[0])

                def product(role):
                    extent = split[role]
                    partial[i] = jnp.dot(
                        lines[here, :extent], landing[j, :extent, :], preferred_element_type=jnp.float32
                    ).astype(jnp.bfloat16)

                on_middle(lambda: product(0))
                on_end(lambda: product(1))
                core_copy(i).start()

            @pl.when(jnp.logical_and(i >= 1, i < total + 1))
            def _():
                m = i - 1
                core_copy(m).wait_recv()
                side_sent[m] = core_sum(m, 1 - chip).astype(jnp.bfloat16)
                side_copy(m).start()

            @pl.when(jnp.logical_and(i >= 3, i < total + 3))
            def _():
                m = i - 3
                j = lax.div(m, 2)
                side_copy(m).wait_recv()
                summed = core_sum(m, chip) + side_got[block, m].astype(jnp.float32)

                @pl.when(lax.rem(m, 2) == 0)
                def _():
                    pair_sent[j] = summed.astype(jnp.bfloat16)
                    pair_copy(j).start()

                @pl.when(lax.rem(m, 2) == 1)
                def _():
                    kept[j] = summed

            @pl.when(jnp.logical_and(i >= 6, even))
            def _():
                j = lax.div(i - 6, 2)
                pair_copy(j).wait_recv()
                residual[j] = residual[j] + factor * (kept[j] + pair_got[block, j].astype(jnp.float32))
                if block < 2:
                    spread_out(block + 1, j)
                else:
                    out[:, pl.ds(aligned(j * LANES, LANES), LANES)] = residual[j].astype(out.dtype)

            if arriving == "last":

                @pl.when(jnp.logical_and(jnp.logical_not(even), i < total - 4))
                def _():
                    j = lax.div(i, 2)
                    pass_on([exit_piece(block, j + 2)], 1)
                    pass_on([exit_piece(block, j + 2)], 2)

            for n, hook in hooks.items():
                pl.when(i == n)(hook)

            return carry

        lax.fori_loop(0, total + 5, step, 0)

        def drain(m, carry):
            core_copy(m).wait_send()
            side_copy(m).wait_send()

            @pl.when(m < quarters)
            def _():
                pair_copy(m).wait_send()

            return carry

        lax.fori_loop(0, total, drain, 0)

    first, later = outof[0][: quarters // 2], outof[0][quarters // 2 :]
    send_near(first)
    send_far(first)
    send_near(into[0])
    send_far(into[0])
    for j in range(quarters):
        residual[j] = tokens[:, j * LANES : (j + 1) * LANES].astype(jnp.float32)
        spread_out(0, j)
    send_near(later)
    for b in range(3):
        start_own(pieces[b])
    send_near(pieces[1] + into[2][:1])
    on_end(lambda: send_near(into[2][1:]))

    for piece in first + into[0]:
        pass_on([piece], 0)
        pass_on([piece], 1)
    send_far(later)
    on_middle(lambda: spread_mate(0), lambda: pass_on(first + into[0], 2))
    on_end(
        lambda: pass_on(first + into[0][:1], 2),
        lambda: spread_mate(0),
        lambda: pass_on(into[0][1:], 2),
    )
    spread_side(0)
    pass_on(later, 0)
    send_far(pieces[1])
    on_middle(lambda: meet(pieces[1], 0))
    send_far(into[2])
    complete(into[0][:1])
    on_middle(lambda: gate_units(0, in_first, 0))
    on_end(lambda: gate_units(0, in_first, 1))
    complete(into[0][1:])
    on_middle(lambda: hidden_units(0, in_first, 0))
    on_end(lambda: hidden_units(0, in_first, 1))
    pass_on(later, 1)
    hooks = {
        5: lambda: on_each(lambda: on_end(lambda: meet(pieces[1], 0)), lambda: twin(pieces[1], 0)),
        7: lambda: pass_on(pieces[1], 1),
        11: lambda: on_each(
            lambda: pass_on(pieces[1], 2),
            lambda: on_middle(lambda: pass_on(into[2], 0)), lambda: on_end(lambda: pass_on(into[2][:1], 0))
        ),
    }
    branch(0, hidden, out_first, 0.5, "late", hooks)

    on_end(lambda: send_near(outof[2]))
    on_middle(lambda: send_near(into[2][1:]))
    spread_mate(1)
    pass_on(into[2][:1], 1)
    spread_side(1)
    complete(pieces[1])
    on_middle(lambda: mixed_rows(1, in_mixer, 0))
    on_end(lambda: mixed_rows(1, in_mixer, 1))

    def exits_over():
        for piece in outof[2]:
            send_far([piece])
            pass_on([piece], 0)

    hooks = {
        4: lambda: pass_on(into[2][1:], 1),
        0: lambda: on_middle(lambda: send_near(outof[2])),
        5: lambda: on_each(lambda: on_middle(exits_over), lambda: on_end(lambda: pass_on(into[2][1:], 0))),
        8: lambda: on_end(lambda: pass_on(outof[2], 0)),
        10: lambda: pass_on(into[2][:1], 2),
    }
    branch(1, mixed, out_mixer, 1.0, "", hooks)

    spread_mate(2)
    pass_on(into[2][1:], 2)
    spread_side(2)
    complete(into[2][:1])
    on_middle(lambda: gate_units(2, in_last, 0))
    on_end(lambda: gate_units(2, in_last, 1))
    pass_on(outof[2][:1], 1)
    pass_on(outof[2][:1], 2)
    complete(into[2][1:])
    on_middle(lambda: hidden_units(2, in_last, 0))
    on_end(lambda: hidden_units(2, in_last, 1))
    pass_on(outof[2][1:2], 1)
    pass_on(outof[2][1:2], 2)
    branch(2, hidden, out_last, 0.5, "last", {})

    for block in range(3):
        spread_sent(block)
        sent(pieces[block])


def pair_shards(
    tokens,
    gain_first,
    gate_first,
    up_first,
    down_first,
    gain_mixer,
    outer_gate,
    inner_gate,
    conv_input,
    conv_taps,
    mixer_out,
    gain_last,
    gate_last,
    up_last,
    down_last,
):
    rows, cols = tokens.shape
    width = gain_first.shape[0]
    quarters, side = cols // LANES, gate_first.shape[0] // 2
    units, held_units = split_shard(gate_first.shape[1])
    channels, held_channels = split_shard(outer_gate.shape[1])
    bf16, f32 = jnp.bfloat16, jnp.float32
    vmem = pl.BlockSpec(memory_space=pltpu.VMEM)
    hbm = pl.BlockSpec(memory_space=pl.ANY)
    dma = pltpu.SemaphoreType.DMA
    count = 7 + 3 * quarters
    return pl.pallas_call(
        layer_kernel,
        name="layer",
        out_shape=jax.ShapeDtypeStruct((rows, cols), bf16),
        in_specs=[vmem] * 5 + [hbm] * 10,
        out_specs=vmem,
        scratch_shapes=[
            pltpu.VMEM((width, 2 * units), bf16),
            pltpu.VMEM((quarters, units, 4 * LANES), bf16),
            pltpu.VMEM((width, 3 * channels), bf16),
            pltpu.VMEM((quarters, channels, 4 * LANES), bf16),
            pltpu.VMEM((width, 2 * units), bf16),
            pltpu.VMEM((quarters, units, 4 * LANES), bf16),
            pltpu.VMEM((3, 2 * rows, width), bf16),
            pltpu.VMEM((2 * rows, units), f32),
            pltpu.VMEM((2 * rows, units), bf16),
            pltpu.VMEM((2 * rows, channels), bf16),
            pltpu.VMEM((2 * quarters, rows, 4 * LANES), bf16),
            pltpu.VMEM((3, 2 * quarters, rows, 2 * LANES), bf16),
            pltpu.VMEM((2 * quarters, rows, LANES), bf16),
            pltpu.VMEM((3, 2 * quarters, rows, LANES), bf16),
            pltpu.VMEM((quarters, rows, LANES), bf16),
            pltpu.VMEM((3, quarters, rows, LANES), bf16),
            pltpu.VMEM((quarters, rows, LANES), f32),
            pltpu.VMEM((quarters, rows, LANES), f32),
            pltpu.VMEM((side, 2 * held_units), bf16),
            pltpu.VMEM((quarters, held_units // 2, LANES), bf16),
            pltpu.VMEM((side, 3 * held_channels), bf16),
            pltpu.VMEM((quarters, held_channels // 2, LANES), bf16),
            pltpu.VMEM((side, 2 * held_units), bf16),
            pltpu.VMEM((quarters, held_units // 2, LANES), bf16),
            dma((count, 3)),
            dma((count, 3)),
            dma((count, 3)),
            dma((count, 3)),
            dma((count, 2)),
            dma((count,)),
            dma((count,)),
            dma((3, 7, quarters)),
            dma((3, 7, quarters)),
            dma((3, 2, 2 * quarters)),
            dma((3, 2, 2 * quarters)),
            dma((3, 2, quarters)),
        ],
        compiler_params=pltpu.CompilerParams(
            collective_id=0, has_side_effects=True, vmem_limit_bytes=VMEM_LIMIT
        ),
    )(
        tokens,
        gain_first[None, :],
        gain_mixer[None, :],
        gain_last[None, :],
        conv_taps,
        gate_first,
        up_first,
        down_first,
        outer_gate,
        inner_gate,
        conv_input,
        mixer_out,
        gate_last,
        up_last,
        down_last,
    )


def solution(mesh):
    in_specs = (
        P(("grp", "fs"), "tp"),
        P(),
        P("fs", "tp"),
        P("fs", "tp"),
        P("tp", "fs"),
        P(),
        P("fs", "tp"),
        P("fs", "tp"),
        P("fs", "tp"),
        P(None, "tp"),
        P("tp", "fs"),
        P(),
        P("fs", "tp"),
        P("fs", "tp"),
        P("tp", "fs"),
    )
    out_specs = P(("grp", "fs"), "tp")
    groups, ring, parts = mesh.shape["grp"], mesh.shape["fs"], mesh.shape["tp"]
    general = make_shards(groups, ring, parts)

    def shards(*args):
        rows, cols = args[0].shape
        depth, units = args[2].shape
        channels = args[6].shape[1]
        fits = (
            groups == 2
            and parts == 4
            and ring == 4
            and rows % SEQ_LEN == 0
            and cols % LANES == 0
            and depth % (groups * LANES) == 0
            and units % (2 * LANES) == 0
            and channels % (2 * LANES) == 0
        )
        return (pair_shards if fits else general)(*args)

    return jax.shard_map(shards, mesh=mesh, in_specs=in_specs, out_specs=out_specs, check_vma=False)
```

```python
import functools

import jax
import jax.numpy as jnp
from jax import lax
from jax.experimental import pallas as pl
from jax.experimental.pallas import tpu as pltpu
from jax.sharding import PartitionSpec as P

SEQ_LEN = 64

VMEM_LIMIT = 63 * 2**20
LANES = 128
MESH = pl.DeviceIdType.MESH

norm_eps = 1e-06


def scaled_rows(residual, gain_vec, inverse):
    return (residual * inverse * gain_vec).astype(jnp.bfloat16)


def causal_mixing(gated, conv_taps):
    row_count, channels = gated.shape
    shaped = gated.reshape(row_count // SEQ_LEN, SEQ_LEN, channels)
    kernel = conv_taps.shape[0]
    padded = jnp.pad(shaped, ((0, 0), (kernel - 1, 0), (0, 0)))
    result = jnp.zeros_like(shaped)
    for offset in range(kernel):
        result = result + conv_taps[offset] * padded[:, offset : offset + SEQ_LEN]
    return result.reshape(row_count, channels)


def make_shards(groups, ring, parts):
    def shift(value, axis, size, by):
        return lax.ppermute(value, axis, [(i, (i + by) % size) for i in range(size)])

    def shards(
        tokens,
        gain_first,
        gate_first,
        up_first,
        down_first,
        gain_mixer,
        outer_gate,
        inner_gate,
        conv_input,
        conv_taps,
        mixer_out,
        gain_last,
        gate_last,
        up_last,
        down_last,
    ):
        column_count = tokens.shape[1]
        width = column_count * parts
        grain = width // (ring * groups)
        g = lax.axis_index("grp")
        z = lax.axis_index("fs")
        t = lax.axis_index("tp")

        def gather(batches, flights):
            pieces = {}
            landed = []
            for batch in batches:
                for name, (weight, axis) in batch.items():
                    pieces[name] = [weight]
                travelling = {
                    name: lax.dynamic_slice_in_dim(weight, g * grain, grain, axis)
                    for name, (weight, axis) in batch.items()
                }
                for _ in range(1, ring):
                    for name in batch:
                        block = travelling[name]
                        if len(landed) >= flights:
                            block, _ = lax.optimization_barrier((block, landed[-flights]))
                        block = shift(block, "fs", ring, 1)
                        landed.append(block)
                        travelling[name] = block
                        pieces[name].append(block)
                        for j in range(1, groups):
                            pieces[name].append(shift(block, "grp", groups, -j))
            return pieces

        def arrival_order(value):
            axis = value.ndim - 1
            blocks = [lax.dynamic_slice_in_dim(value, z * groups * grain, groups * grain, axis)]
            for r in range(1, ring):
                for j in range(groups):
                    start = ((z - r) % ring * groups + (g + j) % groups) * grain
                    blocks.append(lax.dynamic_slice_in_dim(value, start, grain, axis))
            return jnp.concatenate(blocks, axis)

        def own_columns(value, owner):
            blocks = []
            for k in range(column_count // grain):
                block = owner * (column_count // grain) + k
                shard, half = block // groups, block % groups
                turn = (z - shard) % ring
                place = turn * groups + jnp.where(turn == 0, half, (half - g) % groups)
                blocks.append(lax.dynamic_slice_in_dim(value, place * grain, grain, 1))
            return jnp.concatenate(blocks, 1)

        pieces = gather(
            (
                {"gate_first": (gate_first, 0), "up_first": (up_first, 0), "down_first": (down_first, 1)},
                {
                    "entries": (jnp.concatenate((outer_gate, inner_gate, conv_input), 1), 0),
                    "mixer_out": (mixer_out, 1),
                },
                {"gate_last": (gate_last, 0), "up_last": (up_last, 0), "down_last": (down_last, 1)},
            ),
            4,
        )

        def into(normed, pieces):
            total, start = 0.0, 0
            for piece in pieces:
                rows = normed[:, start : start + piece.shape[0]]
                total = total + jnp.dot(rows, piece, preferred_element_type=jnp.float32)
                start += piece.shape[0]
            return total

        def out_of(hidden, pieces):
            return jnp.concatenate(
                [
                    jnp.dot(hidden, piece, preferred_element_type=jnp.float32).astype(
                        jnp.bfloat16
                    )
                    for piece in pieces
                ],
                1,
            )

        def normalize(residual, gain_vec):
            inverse = lax.rsqrt(jnp.mean(residual * residual, axis=1, keepdims=True) + norm_eps)
            return scaled_rows(residual, gain_vec, inverse)

        def hidden_units(normed, gate_pieces, up_pieces):
            gate_pre, up_pre = into(normed, gate_pieces), into(normed, up_pieces)
            return (jax.nn.silu(gate_pre) * up_pre).astype(jnp.bfloat16)

        def add_branch(residual, branch, factor):
            return residual + factor * lax.psum(branch, "tp").astype(jnp.float32)

        residual = arrival_order(lax.all_gather(tokens, "tp", axis=1, tiled=True))
        residual = residual.astype(jnp.float32)

        normed = normalize(residual, arrival_order(gain_first))
        hidden = hidden_units(normed, pieces["gate_first"], pieces["up_first"])
        residual = add_branch(residual, out_of(hidden, pieces["down_first"]), 0.5)

        normed = normalize(residual, arrival_order(gain_mixer))
        channels = pieces["entries"][0].shape[1] // 3
        projected = into(normed, pieces["entries"])
        outer_pre, inner_pre, value_pre = (
            projected[:, i * channels : (i + 1) * channels] for i in range(3)
        )
        convolved = causal_mixing(inner_pre * value_pre, conv_taps)
        mixed_rows = (outer_pre * convolved).astype(jnp.bfloat16)
        residual = add_branch(residual, out_of(mixed_rows, pieces["mixer_out"]), 1.0)

        normed = normalize(residual, arrival_order(gain_last))
        hidden = hidden_units(normed, pieces["gate_last"], pieces["up_last"])
        branch = out_of(hidden, pieces["down_last"])
        total = own_columns(branch, t).astype(jnp.float32)
        for k in range(1, parts):
            theirs = own_columns(branch, (t + k) % parts)
            total = total + shift(theirs, "tp", parts, k).astype(jnp.float32)
        return (own_columns(residual, t) + 0.5 * total).astype(jnp.bfloat16)

    return shards


def split_shard(extent):
    end = max(1, extent // LANES * 2 // 5) * LANES
    return extent - end, end


def layer_kernel(
    tokens,
    gain_first,
    gain_mixer,
    gain_last,
    conv_taps,
    gate_first,
    up_first,
    down_first,
    outer_gate,
    inner_gate,
    conv_input,
    mixer_out,
    gate_last,
    up_last,
    down_last,
    out,
    in_first,
    out_first,
    in_mixer,
    out_mixer,
    in_last,
    out_last,
    spread,
    gated_pre,
    hidden,
    mixed,
    partial,
    core_got,
    side_sent,
    side_got,
    pair_sent,
    pair_got,
    kept,
    residual,
    lift_in_first,
    lift_out_first,
    lift_in_mixer,
    lift_out_mixer,
    lift_in_last,
    lift_out_last,
    weight_sent,
    weight_got,
    twin_sent,
    twin_got,
    relay_sent,
    lift_got,
    own_got,
    token_sent,
    token_got,
    branch_sent,
    core_sems,
    side_sems,
    pair_sems,
):
    g, z, t = lax.axis_index("grp"), lax.axis_index("fs"), lax.axis_index("tp")
    half, pair = lax.rem(z, 2), lax.div(z, 2)
    mate = 2 * pair + 1 - half
    far_middle, far_end = 2 - pair, 3 * (1 - pair)
    middle = half != pair
    chip, core = lax.div(t, 2), lax.rem(t, 2)
    beside = (1 - chip) * 2 + core
    rows, cols = tokens.shape
    quarters = cols // LANES
    depth = gate_first.shape[0]
    to_mate, to_far_middle, to_far_end = (g, mate, t), (g, far_middle, t), (g, far_end, t)
    to_twin, to_side, to_core = (1 - g, z, t), (g, z, beside), (g, z, 2 * chip + 1 - core)

    barrier = pltpu.get_barrier_semaphore()
    peers = (to_mate, to_far_middle, to_far_end, to_twin, to_side, to_core)
    for peer in peers:
        pl.semaphore_signal(barrier, inc=1, device_id=peer, device_id_type=MESH)
    pl.semaphore_wait(barrier, len(peers))

    def remote(src, dst, sent, got, peer):
        return pltpu.make_async_remote_copy(
            src_ref=src, dst_ref=dst, send_sem=sent, recv_sem=got, device_id=peer, device_id_type=MESH
        )

    def aligned(value, unit):
        return pl.multiple_of(value, unit)

    entries = (
        ((gate_first, in_first, 0), (up_first, in_first, 1)),
        ((outer_gate, in_mixer, 0), (inner_gate, in_mixer, 1), (conv_input, in_mixer, 2)),
        ((gate_last, in_last, 0), (up_last, in_last, 1)),
    )
    exits = ((down_first, out_first), (mixer_out, out_mixer), (down_last, out_last))
    lifts = ((lift_in_first, lift_out_first), (lift_in_mixer, lift_out_mixer), (lift_in_last, lift_out_last))
    numbers, exit_base = [], []
    count = 0
    for entry in entries:
        numbers.append(list(range(count, count + len(entry))))
        exit_base.append(count + len(entry))
        count += len(entry) + quarters

    def entry_piece(block, n):
        array, landing, place = entries[block][n]
        split, side = split_shard(array.shape[1]), depth // 2

        def source(role, whole):
            lines = pl.ds(0, depth) if whole else pl.ds(aligned(g * side, side), side)
            return array.at[lines, pl.ds(role * split[0], split[role])]

        def target(role, origin, whole):
            begin = origin * depth if whole else origin * depth + g * side
            return landing.at[
                pl.ds(aligned(begin, side), depth if whole else side), pl.ds(place * split[role], split[role])
            ]

        def three(role):
            return landing.at[pl.ds(0, 3 * side), pl.ds(place * split[role], split[role])]

        hold = lifts[block][0].at[:, pl.ds(place * split[1], split[1])]
        return numbers[block][n], source, target, hold, three

    def exit_piece(block, j):
        array, landing = exits[block]
        split = split_shard(array.shape[0])

        def source(role, whole):
            side = split[role] // 2
            begin = role * split[0] if whole else role * split[0] + g * side
            return array.at[
                pl.ds(begin if whole else aligned(begin, 8), split[role] if whole else side),
                pl.ds(aligned(j * LANES, LANES), LANES),
            ]

        def target(role, origin, whole):
            side = split[role] // 2
            place = lax.rem(origin, 2) * 2 + lax.div(origin, 2)
            lines = pl.ds(0, split[role]) if whole else pl.ds(aligned(g * side, side), side)
            return landing.at[j, lines, pl.ds(aligned(place * LANES, LANES), LANES)]

        def three(role):
            return landing.at[j, pl.ds(0, split[role] // 2), pl.ds(0, 3 * LANES)]

        return exit_base[block] + j, source, target, lifts[block][1].at[j], three

    origins = (mate, far_middle, far_end)

    def on_each(*steps):
        for step in steps:
            step()

    def on_middle(*steps):
        pl.when(middle)(functools.partial(on_each, *steps))

    def on_end(*steps):
        pl.when(jnp.logical_not(middle))(functools.partial(on_each, *steps))

    def mate_middle(piece):
        w, source, target, _, _ = piece
        return remote(source(0, False), target(0, z, False), weight_sent.at[w, 0], weight_got.at[w, 0], to_mate)

    def lift_copy(piece):
        w, source, _, hold, _ = piece
        return remote(source(1, False), hold, weight_sent.at[w, 1], lift_got.at[w], to_mate)

    def mate_end(piece):
        w, source, target, _, _ = piece
        return remote(source(1, False), target(1, z, False), weight_sent.at[w, 0], weight_got.at[w, 0], to_mate)

    def middle_copy(piece):
        w, source, target, _, _ = piece
        return remote(source(0, False), target(0, z, False), weight_sent.at[w, 1], weight_got.at[w, 1], to_far_middle)

    def end_copy(piece):
        w, source, target, _, _ = piece
        return remote(source(1, False), target(1, z, False), weight_sent.at[w, 2], weight_got.at[w, 1], to_far_end)

    def relay_middle(piece):
        w, _, target, _, _ = piece
        view = target(0, mate, False)
        return remote(view, view, relay_sent.at[w, 0], weight_got.at[w, 2], to_far_middle)

    def relay_end(piece):
        w, _, target, hold, _ = piece
        return remote(hold, target(1, mate, False), relay_sent.at[w, 1], weight_got.at[w, 2], to_far_end)

    def twin_copy(piece, role, k):
        w, _, target, _, _ = piece
        view = target(role, origins[k], False)
        return remote(view, view, twin_sent.at[w], twin_got.at[w], to_twin)

    def twins_done(piece, role, semaphores):
        w, _, _, _, three = piece
        pltpu.make_async_copy(three(role), three(role), semaphores.at[w]).wait()

    def own_copy(piece, role):
        w, source, target, _, _ = piece
        return pltpu.make_async_copy(source(role, True), target(role, z, True), own_got.at[w])

    def arrival(piece, role, k):
        w, _, target, _, _ = piece
        view = target(role, origins[k], False)
        return remote(view, view, weight_sent.at[w, 0], weight_got.at[w, k], to_mate)

    def send_near(pieces):
        for piece in pieces:
            on_middle(lambda: mate_end(piece).start())
            on_end(lambda: mate_middle(piece).start(), lambda: lift_copy(piece).start())

    def send_far(pieces):
        @pl.when(middle)
        def _():
            for piece in pieces:
                middle_copy(piece).start()
                end_copy(piece).start()

    def start_own(pieces):
        for piece in pieces:
            on_middle(lambda: own_copy(piece, 0).start())
            on_end(lambda: own_copy(piece, 1).start())

    def meet(pieces, k):
        @pl.when(middle)
        def _():
            for piece in pieces:
                arrival(piece, 0, k).wait_recv()
                if k == 0:
                    relay_middle(piece).start()
                    lift_copy(piece).wait_recv()
                    relay_end(piece).start()

        @pl.when(jnp.logical_not(middle))
        def _():
            for piece in pieces:
                arrival(piece, 1, k).wait_recv()

    def twin(pieces, k):
        for piece in pieces:
            on_middle(lambda: twin_copy(piece, 0, k).start())
            on_end(lambda: twin_copy(piece, 1, k).start())

    def pass_on(pieces, k):
        for piece in pieces:
            meet([piece], k)
            twin([piece], k)

    def complete(pieces):
        @pl.when(middle)
        def _():
            for piece in pieces:
                own_copy(piece, 0).wait()
                twins_done(piece, 0, twin_got)

        @pl.when(jnp.logical_not(middle))
        def _():
            for piece in pieces:
                own_copy(piece, 1).wait()
                twins_done(piece, 1, twin_got)

    def sent(pieces):
        @pl.when(middle)
        def _():
            for piece in pieces:
                for copy in (mate_end, middle_copy, end_copy, relay_middle, relay_end):
                    copy(piece).wait_send()
                twins_done(piece, 0, twin_sent)

        @pl.when(jnp.logical_not(middle))
        def _():
            for piece in pieces:
                for copy in (mate_middle, lift_copy):
                    copy(piece).wait_send()
                twins_done(piece, 1, twin_sent)

    into = [[entry_piece(b, n) for n in range(len(entries[b]))] for b in range(3)]
    outof = [[exit_piece(b, j) for j in range(quarters)] for b in range(3)]
    pieces = [into[b] + outof[b] for b in range(3)]

    def token_copy(block, kind, j):
        column, whose, peer = (
            (t, half, to_mate),
            (t, half, to_side),
            (t, 1 - half, to_side),
            (t, half, to_core),
            (t, 1 - half, to_core),
            (beside, half, to_core),
            (beside, 1 - half, to_core),
        )[kind]
        view = spread.at[
            block,
            pl.ds(aligned(whose * rows, rows), rows),
            pl.ds(aligned(column * cols + j * LANES, LANES), LANES),
        ]
        return remote(view, view, token_sent.at[kind, j], token_got.at[block, kind, j], peer)

    gains = (gain_first, gain_mixer, gain_last)

    def spread_out(block, j):
        place = pl.ds(aligned(t * cols + j * LANES, LANES), LANES)
        spread[block, pl.ds(aligned(half * rows, rows), rows), place] = (
            residual[j] * gains[block][:, place]
        ).astype(jnp.bfloat16)
        for kind in (0, 1, 3):
            token_copy(block, kind, j).start()

    def spread_mate(block):
        for j in range(quarters):
            token_copy(block, 0, j).wait_recv()
            token_copy(block, 2, j).start()
            token_copy(block, 4, j).start()

    def spread_side(block):
        for first, second in ((1, 5), (2, 6)):
            for j in range(quarters):
                token_copy(block, first, j).wait_recv()
                token_copy(block, second, j).start()
        for kind in range(3, 7):
            for j in range(quarters):
                token_copy(block, kind, j).wait_recv()

    def spread_sent(block):
        for kind in range(7):
            for j in range(quarters):
                token_copy(block, kind, j).wait_send()

    def row_factor(lines, gain):
        plain = lines.astype(jnp.float32) * (1.0 / gain[...])
        return lax.rsqrt(jnp.mean(plain * plain, axis=1, keepdims=True) + norm_eps)

    def gate_units(block, landing, role):
        extent = split_shard(gate_first.shape[1])[role]

        def step(i, carry):
            here = pl.ds(aligned(i * rows, rows), rows)
            lines = spread[block, here, :]
            pre = jnp.dot(lines, landing[:, :extent], preferred_element_type=jnp.float32)
            gated_pre[here, :extent] = pre * row_factor(lines, gains[block])
            return carry

        lax.fori_loop(0, 2, step, 0)

    def hidden_units(block, landing, role):
        extent = split_shard(gate_first.shape[1])[role]

        def step(i, carry):
            here = pl.ds(aligned(i * rows, rows), rows)
            lines = spread[block, here, :]
            pre = jnp.dot(lines, landing[:, extent : 2 * extent], preferred_element_type=jnp.float32)
            pre = pre * row_factor(lines, gains[block])
            hidden[here, :extent] = (jax.nn.silu(gated_pre[here, :extent]) * pre).astype(jnp.bfloat16)
            return carry

        lax.fori_loop(0, 2, step, 0)

    def mixed_rows(block, landing, role):
        split = split_shard(conv_taps.shape[1])
        extent = split[role]
        taps = conv_taps[:, role * split[0] : role * split[0] + extent]
        kernel = taps.shape[0]

        def step(i, carry):
            here = pl.ds(aligned(i * rows, rows), rows)
            lines = spread[block, here, :]
            all_pre = jnp.dot(lines, landing[:, : 3 * extent], preferred_element_type=jnp.float32)
            all_pre = all_pre * row_factor(lines, gains[block])
            gated = all_pre[:, extent : 2 * extent] * all_pre[:, 2 * extent : 3 * extent]
            position = lax.rem(lax.broadcasted_iota(jnp.int32, gated.shape, 0), SEQ_LEN)
            convolved = taps[kernel - 1 : kernel, :] * gated
            for back in range(1, kernel):
                moved = jnp.where(position >= back, pltpu.roll(gated, back, 0), 0.0)
                convolved = convolved + taps[kernel - 1 - back : kernel - back, :] * moved
            mixed[here, :extent] = (all_pre[:, :extent] * convolved).astype(jnp.bfloat16)
            return carry

        lax.fori_loop(0, 2, step, 0)

    def branch(block, lines, landing, factor, arriving, hooks):
        def core_copy(m):
            return remote(
                partial.at[m, :, pl.ds(aligned((1 - core) * 2 * LANES, LANES), 2 * LANES)],
                core_got.at[block, m],
                branch_sent.at[0, m],
                core_sems.at[block, m],
                to_core,
            )

        def side_copy(m):
            return remote(
                side_sent.at[m],
                side_got.at[block, m],
                branch_sent.at[1, m],
                side_sems.at[block, m],
                to_side,
            )

        def pair_copy(j):
            return remote(
                pair_sent.at[j],
                pair_got.at[block, j],
                branch_sent.at[2, j],
                pair_sems.at[block, j],
                to_mate,
            )

        def core_sum(m, which):
            mine = partial[m, :, pl.ds(aligned((core * 2 + which) * LANES, LANES), LANES)]
            theirs = core_got[block, m, :, pl.ds(aligned(which * LANES, LANES), LANES)]
            return mine.astype(jnp.float32) + theirs.astype(jnp.float32)

        total = 2 * quarters

        def step(i, carry):
            even = lax.rem(i, 2) == 0

            @pl.when(i < total)
            def _():
                j = lax.div(i, 2)
                if arriving == "late":

                    @pl.when(jnp.logical_and(even, jnp.logical_and(j >= quarters // 2 - 1, j < quarters - 1)))
                    def _():
                        pass_on([exit_piece(block, j + 1)], 2)

                if arriving:

                    @pl.when(even)
                    def _():
                        complete([exit_piece(block, j)])

                whose = lax.rem(lax.rem(i, 2) + 1 - half, 2)
                here = pl.ds(aligned(whose * rows, rows), rows)
                split = split_shard(exits[block][0].shape[0])

                def product(role):
                    extent = split[role]
                    partial[i] = jnp.dot(
                        lines[here, :extent], landing[j, :extent, :], preferred_element_type=jnp.float32
                    ).astype(jnp.bfloat16)

                on_middle(lambda: product(0))
                on_end(lambda: product(1))
                core_copy(i).start()

            @pl.when(jnp.logical_and(i >= 1, i < total + 1))
            def _():
                m = i - 1
                core_copy(m).wait_recv()
                side_sent[m] = core_sum(m, 1 - chip).astype(jnp.bfloat16)
                side_copy(m).start()

            @pl.when(jnp.logical_and(i >= 3, i < total + 3))
            def _():
                m = i - 3
                j = lax.div(m, 2)
                side_copy(m).wait_recv()
                summed = core_sum(m, chip) + side_got[block, m].astype(jnp.float32)

                @pl.when(lax.rem(m, 2) == 0)
                def _():
                    pair_sent[j] = summed.astype(jnp.bfloat16)
                    pair_copy(j).start()

                @pl.when(lax.rem(m, 2) == 1)
                def _():
                    kept[j] = summed

            @pl.when(jnp.logical_and(i >= 6, even))
            def _():
                j = lax.div(i - 6, 2)
                pair_copy(j).wait_recv()
                residual[j] = residual[j] + factor * (kept[j] + pair_got[block, j].astype(jnp.float32))
                if block < 2:
                    spread_out(block + 1, j)
                else:
                    out[:, pl.ds(aligned(j * LANES, LANES), LANES)] = residual[j].astype(out.dtype)

            if arriving == "last":

                @pl.when(jnp.logical_and(jnp.logical_not(even), i < total - 4))
                def _():
                    j = lax.div(i, 2)
                    pass_on([exit_piece(block, j + 2)], 1)
                    pass_on([exit_piece(block, j + 2)], 2)

            for n, hook in hooks.items():
                pl.when(i == n)(hook)

            return carry

        lax.fori_loop(0, total + 5, step, 0)

        def drain(m, carry):
            core_copy(m).wait_send()
            side_copy(m).wait_send()

            @pl.when(m < quarters)
            def _():
                pair_copy(m).wait_send()

            return carry

        lax.fori_loop(0, total, drain, 0)

    first, later = outof[0][: quarters // 2], outof[0][quarters // 2 :]
    send_near(first)
    send_far(first)
    send_near(into[0])
    send_far(into[0])
    for j in range(quarters):
        residual[j] = tokens[:, j * LANES : (j + 1) * LANES].astype(jnp.float32)
        spread_out(0, j)
    send_near(later)
    for b in range(3):
        start_own(pieces[b])
    send_near(pieces[1] + into[2][:1])
    on_end(lambda: send_near(into[2][1:]))

    for piece in first + into[0]:
        pass_on([piece], 0)
        pass_on([piece], 1)
    send_far(later)
    on_middle(lambda: spread_mate(0), lambda: pass_on(first + into[0], 2))
    on_end(
        lambda: pass_on(first + into[0][:1], 2),
        lambda: spread_mate(0),
        lambda: pass_on(into[0][1:], 2),
    )
    spread_side(0)
    pass_on(later, 0)
    send_far(pieces[1])
    on_middle(lambda: meet(pieces[1], 0))
    send_far(into[2])
    complete(into[0][:1])
    on_middle(lambda: gate_units(0, in_first, 0))
    on_end(lambda: gate_units(0, in_first, 1))
    complete(into[0][1:])
    on_middle(lambda: hidden_units(0, in_first, 0))
    on_end(lambda: hidden_units(0, in_first, 1))
    pass_on(later, 1)
    hooks = {
        5: lambda: on_each(lambda: on_end(lambda: meet(pieces[1], 0)), lambda: twin(pieces[1], 0)),
        7: lambda: pass_on(pieces[1], 1),
        11: lambda: on_each(
            lambda: pass_on(pieces[1], 2),
            lambda: on_middle(lambda: pass_on(into[2], 0)), lambda: on_end(lambda: pass_on(into[2][:1], 0))
        ),
    }
    spread_sent(0)
    branch(0, hidden, out_first, 0.5, "late", hooks)

    on_end(lambda: send_near(outof[2]))
    on_middle(lambda: send_near(into[2][1:]))
    spread_mate(1)
    pass_on(into[2][:1], 1)
    spread_side(1)
    complete(pieces[1])
    on_middle(lambda: mixed_rows(1, in_mixer, 0))
    on_end(lambda: mixed_rows(1, in_mixer, 1))

    def exits_over():
        for piece in outof[2]:
            send_far([piece])
            pass_on([piece], 0)

    hooks = {
        4: lambda: pass_on(into[2][1:], 1),
        0: lambda: on_middle(lambda: send_near(outof[2])),
        5: lambda: on_each(lambda: on_middle(exits_over), lambda: on_end(lambda: pass_on(into[2][1:], 0))),
        8: lambda: on_end(lambda: pass_on(outof[2], 0)),
        10: lambda: pass_on(into[2][:1], 2),
    }
    spread_sent(1)
    branch(1, mixed, out_mixer, 1.0, "", hooks)

    spread_mate(2)
    pass_on(into[2][1:], 2)
    spread_side(2)
    complete(into[2][:1])
    on_middle(lambda: gate_units(2, in_last, 0))
    on_end(lambda: gate_units(2, in_last, 1))
    pass_on(outof[2][:1], 1)
    pass_on(outof[2][:1], 2)
    complete(into[2][1:])
    on_middle(lambda: hidden_units(2, in_last, 0))
    on_end(lambda: hidden_units(2, in_last, 1))
    pass_on(outof[2][1:2], 1)
    pass_on(outof[2][1:2], 2)
    spread_sent(2)
    branch(2, hidden, out_last, 0.5, "last", {})

    for block in range(3):
        sent(pieces[block])


def pair_shards(
    tokens,
    gain_first,
    gate_first,
    up_first,
    down_first,
    gain_mixer,
    outer_gate,
    inner_gate,
    conv_input,
    conv_taps,
    mixer_out,
    gain_last,
    gate_last,
    up_last,
    down_last,
):
    rows, cols = tokens.shape
    width = gain_first.shape[0]
    quarters, side = cols // LANES, gate_first.shape[0] // 2
    units, held_units = split_shard(gate_first.shape[1])
    channels, held_channels = split_shard(outer_gate.shape[1])
    bf16, f32 = jnp.bfloat16, jnp.float32
    vmem = pl.BlockSpec(memory_space=pltpu.VMEM)
    hbm = pl.BlockSpec(memory_space=pl.ANY)
    dma = pltpu.SemaphoreType.DMA
    count = 7 + 3 * quarters
    return pl.pallas_call(
        layer_kernel,
        name="layer",
        out_shape=jax.ShapeDtypeStruct((rows, cols), bf16),
        in_specs=[vmem] * 5 + [hbm] * 10,
        out_specs=vmem,
        scratch_shapes=[
            pltpu.VMEM((width, 2 * units), bf16),
            pltpu.VMEM((quarters, units, 4 * LANES), bf16),
            pltpu.VMEM((width, 3 * channels), bf16),
            pltpu.VMEM((quarters, channels, 4 * LANES), bf16),
            pltpu.VMEM((width, 2 * units), bf16),
            pltpu.VMEM((quarters, units, 4 * LANES), bf16),
            pltpu.VMEM((3, 2 * rows, width), bf16),
            pltpu.VMEM((2 * rows, units), f32),
            pltpu.VMEM((2 * rows, units), bf16),
            pltpu.VMEM((2 * rows, channels), bf16),
            pltpu.VMEM((2 * quarters, rows, 4 * LANES), bf16),
            pltpu.VMEM((3, 2 * quarters, rows, 2 * LANES), bf16),
            pltpu.VMEM((2 * quarters, rows, LANES), bf16),
            pltpu.VMEM((3, 2 * quarters, rows, LANES), bf16),
            pltpu.VMEM((quarters, rows, LANES), bf16),
            pltpu.VMEM((3, quarters, rows, LANES), bf16),
            pltpu.VMEM((quarters, rows, LANES), f32),
            pltpu.VMEM((quarters, rows, LANES), f32),
            pltpu.VMEM((side, 2 * held_units), bf16),
            pltpu.VMEM((quarters, held_units // 2, LANES), bf16),
            pltpu.VMEM((side, 3 * held_channels), bf16),
            pltpu.VMEM((quarters, held_channels // 2, LANES), bf16),
            pltpu.VMEM((side, 2 * held_units), bf16),
            pltpu.VMEM((quarters, held_units // 2, LANES), bf16),
            dma((count, 3)),
            dma((count, 3)),
            dma((count,)),
            dma((count,)),
            dma((count, 2)),
            dma((count,)),
            dma((count,)),
            dma((7, quarters)),
            dma((3, 7, quarters)),
            dma((3, 2 * quarters)),
            dma((3, 2 * quarters)),
            dma((3, 2 * quarters)),
            dma((3, quarters)),
        ],
        compiler_params=pltpu.CompilerParams(
            collective_id=0, has_side_effects=True, vmem_limit_bytes=VMEM_LIMIT
        ),
    )(
        tokens,
        gain_first[None, :],
        gain_mixer[None, :],
        gain_last[None, :],
        conv_taps,
        gate_first,
        up_first,
        down_first,
        outer_gate,
        inner_gate,
        conv_input,
        mixer_out,
        gate_last,
        up_last,
        down_last,
    )


def solution(mesh):
    in_specs = (
        P(("grp", "fs"), "tp"),
        P(),
        P("fs", "tp"),
        P("fs", "tp"),
        P("tp", "fs"),
        P(),
        P("fs", "tp"),
        P("fs", "tp"),
        P("fs", "tp"),
        P(None, "tp"),
        P("tp", "fs"),
        P(),
        P("fs", "tp"),
        P("fs", "tp"),
        P("tp", "fs"),
    )
    out_specs = P(("grp", "fs"), "tp")
    groups, ring, parts = mesh.shape["grp"], mesh.shape["fs"], mesh.shape["tp"]
    general = make_shards(groups, ring, parts)

    def shards(*args):
        rows, cols = args[0].shape
        depth, units = args[2].shape
        channels = args[6].shape[1]
        fits = (
            groups == 2
            and parts == 4
            and ring == 4
            and rows % SEQ_LEN == 0
            and cols % LANES == 0
            and depth % (groups * LANES) == 0
            and units % (2 * LANES) == 0
            and channels % (2 * LANES) == 0
        )
        return (pair_shards if fits else general)(*args)

    return jax.shard_map(shards, mesh=mesh, in_specs=in_specs, out_specs=out_specs, check_vma=False)
```
